128 devices in a mesh: sp: 32 (over z, y, core), tp: 4 (over x).
Axes of the slice: x: 4, y: 4, z: 4, core: 2. Of those that a mesh axis runs over, the one named last changes fastest.
Arguments:
- queries: bfloat16 [32768, 1024], P('sp', 'tp'), may hold values from -6 to 6
- keys: bfloat16 [32768, 1024], P('sp', 'tp'), may hold values from -6 to 6
- values: bfloat16 [32768, 1024], P('sp', 'tp'), may hold values from -6 to 6
- gates: bfloat16 [32768, 1024], P('sp', 'tp'), may hold values from -6 to 6
- log_decay: float32 [32768, 8], P('sp', 'tp'), may hold values from -1.6 to 0, as said below
- norm_gain: float32 [8, 128], P('tp'), may hold values from 0.1 to 1.9
- out_weight: bfloat16 [1024, 2048], P('tp'), may hold values from -0.1875 to 0.1875
- resid: bfloat16 [32768, 2048], P(('sp', 'tp')), may hold values from -6 to 6
- post_mix_gain: float32 [2048], replicated, may hold values from 0.1 to 1.9
- pre_ffn_gain: float32 [2048], replicated, may hold values from 0.1 to 1.9
- w_gate: bfloat16 [2048, 5632], P('sp', 'tp'), may hold values from -0.125 to 0.125
- w_up: bfloat16 [2048, 5632], P('sp', 'tp'), may hold values from -0.125 to 0.125
- w_down: bfloat16 [5632, 2048], P('tp', 'sp'), may hold values from -0.078125 to 0.078125
- post_ffn_gain: float32 [2048], replicated, may hold values from 0.1 to 1.9
Outputs:
- updated: bfloat16 [32768, 2048], P(('sp', 'tp'))
The draws below stay inside these ranges and needn't reach their ends.
Inputs may be any that keep to these rules, and one draw needn't show every extreme that they name: `log_decay`: every entry is negative.
All inputs are finite; a program needn't handle non-finite values.
Results may differ from the reference program's by a relative error of at most 0.02.
Values may be sent and summed in bfloat16 or wider, within the bound.
No kernel may reach another device: no remote copies, remote signals or barrier semaphores. Data moves between devices by JAX's collectives and lax.ppermute only.
A program may use at most 128 MiB of HBM per device.

```python
import math
import jax
import jax.numpy as jnp
from jax import lax

D = 2048
RETENTION_HEADS = 8
HEAD_DIM = 128
FF = 5632
TOK_DEV = 1024
RET_W = 1024
BLOCK = 512
SEQUENCE_TOKENS = 32768
N_TP = 4


def draw_log_decay(key, part):
    random_child_keys = jax.random.split(jax.random.fold_in(key, 17), 6)
    fast_share = 0.5
    is_fast = jax.random.uniform(random_child_keys[0], (RETENTION_HEADS,), jnp.float32) < fast_share
    fast_rate = jax.random.uniform(random_child_keys[1], (RETENTION_HEADS,), jnp.float32, 0.08, 0.15)
    baseline_decay_rate = jnp.where(is_fast, fast_rate, 0.6 / SEQUENCE_TOKENS)
    span_count = SEQUENCE_TOKENS // TOK_DEV
    factor = jnp.exp(jax.random.uniform(random_child_keys[2], (span_count, RETENTION_HEADS), jnp.float32, math.log(0.4), math.log(1.6)))
    row_values = jnp.repeat(factor, TOK_DEV, axis=0)
    random_noise = jax.random.uniform(random_child_keys[3], (SEQUENCE_TOKENS, RETENTION_HEADS), jnp.float32, 0.5, 1.5)
    spike_position = jax.random.randint(random_child_keys[4], (2, RETENTION_HEADS), 0, SEQUENCE_TOKENS)
    spike_length = jnp.log(jax.random.uniform(random_child_keys[5], (2, RETENTION_HEADS), jnp.float32, 0.55, 0.8))
    token_positions = lax.broadcasted_iota(jnp.int32, (SEQUENCE_TOKENS, RETENTION_HEADS), 0)
    spike_events = jnp.where(token_positions == spike_position[0][None, :], spike_length[0][None, :], 0.0)
    spike_events = spike_events + jnp.where(token_positions == spike_position[1][None, :], spike_length[1][None, :], 0.0)
    return (-baseline_decay_rate[None, :] * row_values * random_noise + spike_events).astype(jnp.float32)


def steps_of(own_key, extent, shards, low, largest):
    loudness, own = 1.0, jax.random.fold_in(own_key, 6)
    for axis_at, blocks in shards:
        draws = jnp.exp(jax.random.uniform(jax.random.fold_in(own, axis_at), (blocks,), jnp.float32, low / len(shards), largest / len(shards)))
        loudness = loudness * jnp.repeat(draws, extent[axis_at] // blocks).reshape([-1 if axis == axis_at else 1 for axis in range(len(extent))])
    return loudness


def normal_values(own_key, shape, spread, reach, cuts=(), dtype=jnp.bfloat16):
    result = spread * jax.random.normal(own_key, shape, jnp.float32)
    if cuts:
        result = result * steps_of(own_key, shape, cuts, -0.22, 0.18)
    return jnp.clip(result, -reach, reach).astype(dtype)


def setup_inputs(seed: int = 0) -> dict:
    streams_of = jax.random.split(jax.random.key(seed), 15)
    return {
        "queries": normal_values(streams_of[0], (SEQUENCE_TOKENS, RET_W), 1.0, 6.0, ((0, 32), (1, 4))),
        "keys": normal_values(streams_of[1], (SEQUENCE_TOKENS, RET_W), 1.0, 6.0, ((0, 32), (1, 4))),
        "values": normal_values(streams_of[2], (SEQUENCE_TOKENS, RET_W), 1.0, 6.0, ((0, 32), (1, 4))),
        "gates": normal_values(streams_of[3], (SEQUENCE_TOKENS, RET_W), 1.0, 6.0, ((0, 32), (1, 4))),
        "log_decay": draw_log_decay(jax.random.fold_in(streams_of[14], 71), 0),
        "norm_gain": jnp.clip(1.0 + 0.18 * jax.random.normal(streams_of[5], (RETENTION_HEADS, HEAD_DIM), jnp.float32), 0.1, 1.9),
        "out_weight": normal_values(streams_of[6], (RET_W, D), RET_W ** -0.5, 0.1875, ((0, 4),)),
        "resid": normal_values(streams_of[7], (SEQUENCE_TOKENS, D), 1.0, 6.0, ((0, 128),)),
        "post_mix_gain": jnp.clip(1.0 + 0.18 * jax.random.normal(streams_of[8], (D,), jnp.float32), 0.1, 1.9),
        "pre_ffn_gain": jnp.clip(1.0 + 0.18 * jax.random.normal(streams_of[9], (D,), jnp.float32), 0.1, 1.9),
        "w_gate": normal_values(streams_of[10], (D, FF), D ** -0.5, 0.125, ((0, 32), (1, 4))),
        "w_up": normal_values(streams_of[11], (D, FF), D ** -0.5, 0.125, ((0, 32), (1, 4))),
        "w_down": normal_values(streams_of[12], (FF, D), FF ** -0.5, 0.078125, ((0, 4), (1, 32))),
        "post_ffn_gain": jnp.clip(1.0 + 0.18 * jax.random.normal(streams_of[13], (D,), jnp.float32), 0.1, 1.9),
    }


EPSILON = 1e-06

def rms_norm(values_in, gain_vec):
    widened = values_in.astype(jnp.float32)
    return widened * lax.rsqrt(lax.optimization_barrier(jnp.mean(widened * widened, axis=-1, keepdims=True)) + EPSILON) * gain_vec.astype(jnp.float32)

def block_step(carried, pieces):
    query_blk, key_blk, value_blk, decay_blk = pieces
    length = query_blk.shape[1]
    key_scale = query_blk.shape[2] ** (-0.5)
    query_wide = query_blk.astype(jnp.float32)
    key_wide = key_blk.astype(jnp.float32)
    value_wide = value_blk.astype(jnp.float32)
    cumulative = jnp.cumsum(decay_blk, axis=1)
    log_gap = cumulative[:, :, None] - cumulative[:, None, :]
    causal = lax.broadcasted_iota(jnp.int32, (length, length), 0) >= lax.broadcasted_iota(jnp.int32, (length, length), 1)
    weight = jnp.where(causal[None], jnp.exp(jnp.minimum(log_gap, 0.0)), 0.0)
    products = jnp.einsum('htd,hsd->hts', query_wide, key_wide)
    scores = lax.optimization_barrier((products * key_scale * weight).astype(jnp.bfloat16))
    within = jnp.einsum('hts,hsd->htd', scores.astype(jnp.float32), value_wide)
    carried_term = jnp.einsum('htd,hde->hte', query_wide, carried, precision=lax.Precision.HIGHEST) * jnp.exp(cumulative)[:, :, None]
    to_end = jnp.exp(cumulative[:, -1:] - cumulative) * key_scale
    scaled_keys = lax.optimization_barrier((key_wide * to_end[:, :, None]).astype(jnp.bfloat16))
    added = jnp.einsum('hsd,hse->hde', scaled_keys.astype(jnp.float32), value_wide)
    carried = jnp.exp(cumulative[:, -1])[:, None, None] * carried + added
    return (carried, within + carried_term)

def to_blocks(matrix, block_len, head_count):
    row_count = matrix.shape[0]
    return matrix.reshape(row_count // block_len, block_len, head_count, -1).transpose(0, 2, 1, 3)

def finish_heads(retention, gates, norm_gain):
    centered = retention - lax.optimization_barrier(jnp.mean(retention, axis=-1, keepdims=True))
    variance = lax.optimization_barrier(jnp.mean(centered * centered, axis=-1, keepdims=True))
    normed = centered * lax.rsqrt(variance + EPSILON) * norm_gain.astype(jnp.float32)[None]
    gate_vals = gates.astype(jnp.float32).reshape(normed.shape)
    return (jax.nn.silu(gate_vals) * normed).reshape(normed.shape[0], -1).astype(jnp.bfloat16)

def grouped_product(left, right, group_count):
    inner = left.shape[1] // group_count
    total = jnp.zeros((left.shape[0], right.shape[1]), jnp.float32)
    for group in range(group_count):
        part = jnp.dot(left[:, group * inner:(group + 1) * inner], right[group * inner:(group + 1) * inner], preferred_element_type=jnp.float32)
        total = total + part.astype(jnp.bfloat16).astype(jnp.float32)
    return total.astype(jnp.bfloat16)

def reference(queries, keys, values, gates, log_decay, norm_gain, out_weight, resid, post_mix_gain, pre_ffn_gain, w_gate, w_up, w_down, post_ffn_gain):
    block_count = SEQUENCE_TOKENS // BLOCK
    query_blocks = to_blocks(queries, BLOCK, RETENTION_HEADS)
    key_blocks = to_blocks(keys, BLOCK, RETENTION_HEADS)
    value_blocks = to_blocks(values, BLOCK, RETENTION_HEADS)
    decay_blocks = log_decay.reshape(block_count, BLOCK, RETENTION_HEADS).transpose(0, 2, 1)
    start_state = jnp.zeros((RETENTION_HEADS, HEAD_DIM, HEAD_DIM), jnp.float32)
    _, outputs = lax.scan(block_step, start_state, (query_blocks, key_blocks, value_blocks, decay_blocks))
    retention = outputs.transpose(0, 2, 1, 3).reshape(SEQUENCE_TOKENS, RETENTION_HEADS, HEAD_DIM)
    retained = finish_heads(retention, gates, norm_gain)
    mixed = grouped_product(retained, out_weight, N_TP)
    middle = (resid.astype(jnp.float32) + rms_norm(mixed, post_mix_gain)).astype(jnp.bfloat16)
    ffn_input = rms_norm(middle, pre_ffn_gain).astype(jnp.bfloat16)

    def ffn_rows(row_block):
        gate_act = jnp.dot(row_block, w_gate, preferred_element_type=jnp.float32)
        up_act = jnp.dot(row_block, w_up, preferred_element_type=jnp.float32)
        hidden = (jax.nn.silu(gate_act) * up_act).astype(jnp.bfloat16)
        return grouped_product(hidden, w_down, N_TP)
    branch = lax.map(ffn_rows, ffn_input.reshape(SEQUENCE_TOKENS // TOK_DEV, TOK_DEV, D)).reshape(SEQUENCE_TOKENS, D)
    return (middle.astype(jnp.float32) + rms_norm(branch, post_ffn_gain)).astype(jnp.bfloat16)
```

```python
import functools

import jax
import jax.numpy as jnp
from jax import lax
from jax.experimental import pallas as pl
from jax.experimental.pallas import tpu as pltpu
from jax.sharding import Mesh
from jax.sharding import PartitionSpec as P

BLOCK = 512
SP = ("sp_0", "sp_1", "sp_2")
SP_TP = ("sp_0", "sp_1", "sp_2", "tp")
RING = 4
EPSILON = 1e-06


def along(axis, step):
    return [(i, (i + step) % RING) for i in range(RING)]


def role_shift(first, step):
    pairs = []
    for z in range(RING):
        for y in range(RING):
            for c in range(2):
                if (c == 0) == first:
                    to = (z, (y + step) % RING)
                else:
                    to = ((z + step) % RING, y)
                pairs.append((z * 8 + y * 2 + c, to[0] * 8 + to[1] * 2 + c))
    return pairs


def swap_cores(x):
    return lax.ppermute(x, "sp_2", [(0, 1), (1, 0)])


def gather_weights(w_gate, w_up, w_down, core):
    pack = jnp.stack([w_gate, w_up, w_down.T])
    half = pack.shape[1] // 2
    keep = lax.dynamic_slice_in_dim(pack, core * half, half, 1)
    give = lax.dynamic_slice_in_dim(pack, (1 - core) * half, half, 1)
    got = swap_cores(give)
    is0 = core == 0
    mine = jnp.stack([jnp.where(is0, keep, got), jnp.where(is0, got, keep)], axis=1)
    quarter = half // 2
    p1 = functools.partial(lax.ppermute, axis_name=SP)
    right = p1(mine, perm=role_shift(True, 1))
    left = p1(mine, perm=role_shift(True, -1))
    far_a = p1(right[:, :, :quarter], perm=role_shift(True, 1))
    far_b = p1(left[:, :, quarter:], perm=role_shift(True, -1))
    s = jnp.stack([mine, right, left, jnp.concatenate([far_a, far_b], axis=2)])
    right2 = p1(s, perm=role_shift(False, 1))
    left2 = p1(s, perm=role_shift(False, -1))
    far2_a = p1(right2[:2], perm=role_shift(False, 1))
    far2_b = p1(left2[2:], perm=role_shift(False, -1))
    own = [s, right2, left2, far2_a, far2_b]
    return own + [swap_cores(v) for v in own]


def ffn_body(n_in, n_out, coord, *refs):
    xs = refs[:n_in]
    pieces = refs[n_in : n_in + 10]
    outs = refs[n_in + 10 : n_in + 10 + n_out]
    w, x, gate, up, hid, sem_gu, sem_d = refs[n_in + 10 + n_out :]
    z, y, c = coord[0], coord[1], coord[2]
    offs = (0, RING - 1, 1, 2)
    plan = []
    for side in range(2):
        color = c if side == 0 else 1 - c
        for group in range(5):
            offg = offs[min(group, 3)]
            count = 4 if group < 3 else 2
            base = 2 if group == 4 else 0
            for k in range(count):
                offj = offs[base + k]
                yy0, zz0 = (y + offj) % RING, (z + offg) % RING
                yy1, zz1 = (y + offg) % RING, (z + offj) % RING
                yy = jnp.where(color == 0, yy0, yy1)
                zz = jnp.where(color == 0, zz0, zz1)
                plan.append((pieces[side * 5 + group], k, color, zz * RING + yy))

    def gu_copy(src, k, color, chip):
        return pltpu.make_async_copy(
            src.at[k, pl.ds(0, 2)], w.at[pl.ds(0, 2), chip, :, color], sem_gu.at[color, chip]
        )

    def d_copy(src, k, color, chip):
        return pltpu.make_async_copy(src.at[k, 2], w.at[2, chip, :, color], sem_d.at[color, chip])

    for item in plan:
        gu_copy(*item).start()
    for item in plan:
        d_copy(*item).start()
    rows = x.shape[0]
    per = rows // n_in
    for i in range(n_in):
        x[i * per : (i + 1) * per, :] = xs[i][...]
    depth = 512
    width = gate.shape[1]

    def load(which, k):
        return w[which, pl.ds(4 * k, 4)].reshape(depth, width)

    for k in range(RING):
        for color in range(2):
            for j in range(4):
                gu_copy(pieces[0], 0, color, 4 * k + j).wait()
        xk = x[:, k * depth : (k + 1) * depth]
        g = jnp.dot(xk, load(0, k), preferred_element_type=jnp.float32)
        u = jnp.dot(xk, load(1, k), preferred_element_type=jnp.float32)
        if k == 0:
            gate[...] = g
            up[...] = u
        elif k < RING - 1:
            gate[...] += g
            up[...] += u
        else:
            g = gate[...] + g
            u = up[...] + u
            hid[...] = (g * (1.0 / (1.0 + jnp.exp(-g))) * u).astype(jnp.bfloat16)
    per_out = rows // n_out
    for k in range(RING):
        for color in range(2):
            for j in range(4):
                d_copy(pieces[0], 0, color, 4 * k + j).wait()
        part = lax.dot_general(
            hid[...], load(2, k), (((1,), (1,)), ((), ())), preferred_element_type=jnp.float32
        ).astype(jnp.bfloat16)
        for i in range(n_out):
            outs[i][:, k * depth : (k + 1) * depth] = part[i * per_out : (i + 1) * per_out]


def ffn(coord, weights, xs, n_out):
    rows = sum(v.shape[0] for v in xs)
    model = xs[0].shape[1]
    width = weights[0].shape[-1]
    vm = pl.BlockSpec(memory_space=pltpu.VMEM)
    hb = pl.BlockSpec(memory_space=pl.ANY)
    flops = 6 * rows * model * width
    return pl.pallas_call(
        functools.partial(ffn_body, len(xs), n_out),
        out_shape=[jax.ShapeDtypeStruct((rows // n_out, model), jnp.bfloat16)] * n_out,
        in_specs=[pl.BlockSpec(memory_space=pltpu.SMEM)] + [vm] * len(xs) + [hb] * 10,
        out_specs=[vm] * n_out,
        scratch_shapes=[
            pltpu.VMEM((3, 16, 2, 2, 32, width), jnp.bfloat16),
            pltpu.VMEM((rows, model), jnp.bfloat16),
            pltpu.VMEM((rows, width), jnp.float32),
            pltpu.VMEM((rows, width), jnp.float32),
            pltpu.VMEM((rows, width), jnp.bfloat16),
            pltpu.SemaphoreType.DMA((2, 16)),
            pltpu.SemaphoreType.DMA((2, 16)),
        ],
        compiler_params=pltpu.CompilerParams(vmem_limit_bytes=48 * 1024 * 1024),
        cost_estimate=pl.CostEstimate(
            flops=flops, bytes_accessed=6 * model * width, transcendentals=rows * width
        ),
        name="ffn_rows",
    )(coord, *xs, *weights)


def rms_norm(values_in, gain_vec):
    widened = values_in.astype(jnp.float32)
    return (
        widened
        * lax.rsqrt(jnp.mean(widened * widened, axis=-1, keepdims=True) + EPSILON)
        * gain_vec
    )


def block_step(carried, pieces):
    query_blk, key_blk, value_blk, decay_blk = pieces
    length = query_blk.shape[1]
    key_scale = query_blk.shape[2] ** (-0.5)
    cumulative = jnp.cumsum(decay_blk, axis=1)
    log_gap = cumulative[:, :, None] - cumulative[:, None, :]
    causal = lax.broadcasted_iota(jnp.int32, (length, length), 0) >= lax.broadcasted_iota(
        jnp.int32, (length, length), 1
    )
    weight = jnp.where(causal[None], jnp.exp(jnp.minimum(log_gap, 0.0)), 0.0)
    products = jnp.einsum("htd,hsd->hts", query_blk, key_blk, preferred_element_type=jnp.float32)
    scores = (products * key_scale * weight).astype(jnp.bfloat16)
    within = jnp.einsum("hts,hsd->htd", scores, value_blk, preferred_element_type=jnp.float32)
    carried_term = (
        jnp.einsum(
            "htd,hde->hte", query_blk.astype(jnp.float32), carried, precision=lax.Precision.HIGHEST
        )
        * jnp.exp(cumulative)[:, :, None]
    )
    to_end = jnp.exp(cumulative[:, -1:] - cumulative) * key_scale
    scaled_keys = (key_blk.astype(jnp.float32) * to_end[:, :, None]).astype(jnp.bfloat16)
    added = jnp.einsum("hsd,hse->hde", scaled_keys, value_blk, preferred_element_type=jnp.float32)
    carried = jnp.exp(cumulative[:, -1])[:, None, None] * carried + added
    return (carried, within + carried_term)


def to_blocks(matrix, block_len, head_count):
    row_count = matrix.shape[0]
    return matrix.reshape(row_count // block_len, block_len, head_count, -1).transpose(0, 2, 1, 3)


def finish_heads(retention, gates, norm_gain):
    centered = retention - jnp.mean(retention, axis=-1, keepdims=True)
    variance = jnp.mean(centered * centered, axis=-1, keepdims=True)
    normed = centered * lax.rsqrt(variance + EPSILON) * norm_gain[None]
    gate_vals = gates.astype(jnp.float32).reshape(normed.shape)
    return (jax.nn.silu(gate_vals) * normed).reshape(normed.shape[0], -1).astype(jnp.bfloat16)


def combine(earlier, later):
    return (earlier[0] * later[0], later[0][:, None, None] * earlier[1] + later[1])


def packed(decay, state):
    high = decay.astype(jnp.bfloat16)
    low = (decay - high.astype(jnp.float32)).astype(jnp.bfloat16)
    row = lax.broadcasted_iota(jnp.int32, (decay.shape[0], 16, state.shape[2]), 1)
    tail = jnp.where(row == 0, high[:, None, None], low[:, None, None])
    return jnp.concatenate([state.astype(jnp.bfloat16), tail], axis=1)


def unpacked(message, depth):
    wide = message.astype(jnp.float32)
    return (wide[:, depth, 0] + wide[:, depth + 1, 0], wide[:, :depth])


def picked(flag, one, other):
    return jax.tree.map(lambda a, b: jnp.where(flag, a, b), one, other)


def entering(decay, state):
    depth = state.shape[1]
    nothing = (jnp.ones_like(decay), jnp.zeros_like(state))
    z, y, c = (lax.axis_index(a) for a in SP)
    message = packed(decay, state)
    mine = unpacked(message, depth)
    other = unpacked(swap_cores(message), depth)
    first = picked(c == 0, mine, other)
    second = picked(c == 0, other, mine)
    core_before = picked(c == 0, nothing, first)
    pair = combine(first, second)
    message = packed(*pair)
    near = [unpacked(message, depth)]
    near += [unpacked(lax.ppermute(message, "sp_1", along("sp_1", k)), depth) for k in (1, 2, 3)]
    total, y_before = nothing, nothing
    for k in range(RING):
        item = near[0]
        for j in range(1, RING):
            item = picked((y - j) % RING == k, near[j], item)
        y_before = picked(y == k, total, y_before)
        total = combine(total, item)
    message = packed(*total)
    z_before = nothing
    for k in (3, 2, 1):
        got = unpacked(
            lax.ppermute(message, "sp_0", [(i, i + k) for i in range(RING - k)]), depth
        )
        z_before = combine(z_before, picked(z >= k, got, nothing))
    return combine(combine(z_before, y_before), core_before)[1]


def ring_rows(v):
    half = v.shape[0] // 2
    right = lax.ppermute(v, "tp", along("tp", 1))
    left = lax.ppermute(v, "tp", along("tp", -1))
    far_a = lax.ppermute(right[:half], "tp", along("tp", 1))
    far_b = lax.ppermute(left[half:], "tp", along("tp", -1))
    return right, left, far_a, far_b


def per_device(
    queries,
    keys,
    values,
    gates,
    log_decay,
    norm_gain,
    out_weight,
    resid,
    post_mix_gain,
    pre_ffn_gain,
    w_gate,
    w_up,
    w_down,
    post_ffn_gain,
):
    z, y, c = (lax.axis_index(a) for a in SP)
    x = lax.axis_index("tp")
    coord = jnp.stack([z, y, c, x]).astype(jnp.int32)
    weights = gather_weights(w_gate, w_up, w_down, c)
    mix_right, mix_left, mix_far_a, mix_far_b = ring_rows(out_weight)
    mix_far = jnp.concatenate([mix_far_a, mix_far_b])

    row_count = queries.shape[0]
    head_count = log_decay.shape[1]
    head_dim = queries.shape[1] // head_count
    block_count = row_count // BLOCK
    query_blocks = to_blocks(queries, BLOCK, head_count)
    key_blocks = to_blocks(keys, BLOCK, head_count)
    value_blocks = to_blocks(values, BLOCK, head_count)
    decay_blocks = log_decay.reshape(block_count, BLOCK, head_count).transpose(0, 2, 1)
    start_state = jnp.zeros((head_count, head_dim, head_dim), jnp.float32)
    local_state, outputs = lax.scan(
        block_step, start_state, (query_blocks, key_blocks, value_blocks, decay_blocks)
    )
    retention = outputs.transpose(0, 2, 1, 3).reshape(row_count, head_count, head_dim)
    cumulative = jnp.cumsum(log_decay, axis=0)
    local_decay = jnp.exp(cumulative[-1])
    incoming = entering(local_decay, local_state)
    query_rows = queries.reshape(row_count, head_count, head_dim).astype(jnp.float32)
    retention = (
        retention
        + jnp.einsum("thd,hde->the", query_rows, incoming, precision=lax.Precision.HIGHEST)
        * jnp.exp(cumulative)[:, :, None]
    )
    retained = finish_heads(retention, gates, norm_gain)
    quarter = resid.shape[0]
    regrouped = lax.all_to_all(retained, "tp", split_axis=0, concat_axis=1, tiled=True)
    group_rows = out_weight.shape[0]
    running = jnp.zeros((quarter, out_weight.shape[1]), jnp.float32)
    for off, piece in ((0, out_weight), (-1, mix_right), (1, mix_left), (2, mix_far)):
        columns = lax.dynamic_slice_in_dim(
            regrouped, ((x + off) % RING) * group_rows, group_rows, 1
        )
        part = jnp.dot(columns, piece, preferred_element_type=jnp.float32)
        running = running + part.astype(jnp.bfloat16).astype(jnp.float32)
    mixed = running.astype(jnp.bfloat16)
    middle = (resid.astype(jnp.float32) + rms_norm(mixed, post_mix_gain)).astype(jnp.bfloat16)
    ffn_input = rms_norm(middle, pre_ffn_gain).astype(jnp.bfloat16)

    right, left, far_a, far_b = ring_rows(ffn_input)
    own_a, own_b = ffn(coord, weights, [ffn_input], 2)
    right_a, right_b = ffn(coord, weights, [right], 2)
    left_a, left_b = ffn(coord, weights, [left], 2)
    opp_a, opp_b = ffn(coord, weights, [far_a, far_b], 2)
    up1, down1 = along("tp", 1), along("tp", -1)
    wide = lambda v: v.astype(jnp.float32)
    from_left_b = lax.ppermute(left_b, "tp", up1)
    from_right_a = lax.ppermute(right_a, "tp", down1)
    far_in_a = lax.ppermute(opp_a, "tp", up1)
    far_in_b = lax.ppermute(opp_b, "tp", down1)
    sum_a = lax.ppermute((wide(left_a) + wide(far_in_a)).astype(jnp.bfloat16), "tp", up1)
    sum_b = lax.ppermute((wide(right_b) + wide(far_in_b)).astype(jnp.bfloat16), "tp", down1)
    branch = jnp.concatenate(
        [wide(own_a) + wide(sum_a) + wide(from_right_a), wide(own_b) + wide(from_left_b) + wide(sum_b)]
    ).astype(jnp.bfloat16)
    return (middle.astype(jnp.float32) + rms_norm(branch, post_ffn_gain)).astype(jnp.bfloat16)


def solution(mesh):
    split = Mesh(mesh.devices.reshape(4, 4, 2, mesh.shape["tp"]), ("sp_0", "sp_1", "sp_2", "tp"))
    placed = (
        P(SP, "tp"),
        P(SP, "tp"),
        P(SP, "tp"),
        P(SP, "tp"),
        P(SP, "tp"),
        P("tp", None),
        P("tp", None),
        P(SP_TP, None),
        P(),
        P(),
        P(SP, "tp"),
        P(SP, "tp"),
        P("tp", SP),
        P(),
    )
    return jax.shard_map(
        per_device, mesh=split, in_specs=placed, out_specs=P(SP_TP, None), check_vma=False
    )
```

```python
import functools

import jax
import jax.numpy as jnp
from jax import lax
from jax.experimental import pallas as pl
from jax.experimental.pallas import tpu as pltpu
from jax.sharding import Mesh
from jax.sharding import PartitionSpec as P


BLOCK = 512
SP = ("sp_0", "sp_1", "sp_2")
SP_TP = ("sp_0", "sp_1", "sp_2", "tp")
RING = 4
EPSILON = 1e-06


def along(step):
    return [(i, (i + step) % RING) for i in range(RING)]


def role_shift(first, step):
    pairs = []
    for z in range(RING):
        for y in range(RING):
            for c in range(2):
                if (c == 0) == first:
                    to = (z, (y + step) % RING)
                else:
                    to = ((z + step) % RING, y)
                pairs.append((z * 8 + y * 2 + c, to[0] * 8 + to[1] * 2 + c))
    return pairs


def flipped(size, bit):
    return [(i, i ^ bit) for i in range(size)]


def gather_weights(w_gate, w_up, w_down):
    mine = jnp.stack([w_gate, w_up, w_down.T])
    near = functools.partial(role_shift, True)
    wide = functools.partial(role_shift, False)
    right = lax.ppermute(mine, SP, near(1))
    left = lax.ppermute(mine, SP, near(-1))
    far = lax.ppermute(mine, SP, near(2))
    s0 = jnp.stack([mine, right])
    s1 = jnp.stack([left, far])
    ra = lax.ppermute(s0, SP, wide(1))
    lb = lax.ppermute(s1, SP, wide(-1))
    fa = lax.ppermute(ra, SP, wide(1))
    fb = lax.ppermute(lb, SP, wide(-1))
    rb = lax.ppermute(s1, SP, wide(1))
    la = lax.ppermute(s0, SP, wide(-1))
    own = [s0, s1, ra, lb, fa, fb, rb, la]
    return own + [lax.ppermute(v, "sp_2", flipped(2, 1)) for v in own]


PIECES = ((0, 0), (2, 0), (0, 3), (2, 1), (0, 2), (2, 2), (2, 3), (0, 1))


def ffn_body(n_in, n_out, coord, *refs):
    xs = refs[:n_in]
    count = 2 * len(PIECES)
    pieces = refs[n_in : n_in + count]
    outs = refs[n_in + count : n_in + count + n_out]
    w, x, gate, up, hid, sem_gu, sem_d = refs[n_in + count + n_out :]
    z, y, c = coord[0], coord[1], coord[2]
    offs = (0, RING - 1, 1, 2)

    def plan(low):
        items = []
        for side in range(2):
            core = side if low else 1 - side
            for i, (first, away) in enumerate(PIECES):
                for k in range(2):
                    near = offs[first + k]
                    dz, dy = (away, near) if core == 0 else (near, away)
                    chip = ((z + dz) % RING) * RING + (y + dy) % RING
                    items.append((dz, pieces[side * len(PIECES) + i], k, core, chip))
        return [item[1:] for item in sorted(items, key=lambda item: item[0])]

    def gu_copy(src, k, core, chip):
        return pltpu.make_async_copy(
            src.at[k, pl.ds(0, 2)], w.at[pl.ds(0, 2), chip, core], sem_gu.at[core, chip]
        )

    def d_copy(src, k, core, chip):
        return pltpu.make_async_copy(src.at[k, 2], w.at[2, chip, core], sem_d.at[core, chip])

    for low in (True, False):

        @pl.when((c == 0) == low)
        def _():
            items = plan(low)
            for item in items:
                gu_copy(*item).start()
            for item in items:
                d_copy(*item).start()

    rows = x.shape[0]
    per = rows // n_in
    for i in range(n_in):
        x[i * per : (i + 1) * per, :] = xs[i][...]
    gate[...] = jnp.zeros_like(gate)
    up[...] = jnp.zeros_like(up)
    depth = 512
    width = gate.shape[1]

    def load(which, k):
        return w[which, pl.ds(4 * k, 4)].reshape(depth, width)

    def enter(step, carry):
        k = (z + step) % RING
        for core in range(2):
            for j in range(4):
                gu_copy(pieces[0], 0, core, 4 * k + j).wait()
        xk = x[:, pl.ds(pl.multiple_of(k * depth, depth), depth)]
        gate[...] += jnp.dot(xk, load(0, k), preferred_element_type=jnp.float32)
        up[...] += jnp.dot(xk, load(1, k), preferred_element_type=jnp.float32)
        return carry

    lax.fori_loop(0, RING, enter, 0)
    g = gate[...]
    hid[...] = (g * (1.0 / (1.0 + jnp.exp(-g))) * up[...]).astype(jnp.bfloat16)
    per_out = rows // n_out

    def leave(step, carry):
        k = (z + step) % RING
        for core in range(2):
            for j in range(4):
                d_copy(pieces[0], 0, core, 4 * k + j).wait()
        part = lax.dot_general(
            hid[...], load(2, k), (((1,), (1,)), ((), ())), preferred_element_type=jnp.float32
        ).astype(jnp.bfloat16)
        for i in range(n_out):
            outs[i][:, pl.ds(pl.multiple_of(k * depth, depth), depth)] = part[
                i * per_out : (i + 1) * per_out
            ]
        return carry

    lax.fori_loop(0, RING, leave, 0)


def ffn(coord, weights, xs, n_out):
    rows = sum(v.shape[0] for v in xs)
    model = xs[0].shape[1]
    width = weights[0].shape[-1]
    vm = pl.BlockSpec(memory_space=pltpu.VMEM)
    hb = pl.BlockSpec(memory_space=pltpu.HBM)
    flops = 6 * rows * model * width
    return pl.pallas_call(
        functools.partial(ffn_body, len(xs), n_out),
        out_shape=[jax.ShapeDtypeStruct((rows // n_out, model), jnp.bfloat16)] * n_out,
        in_specs=[pl.BlockSpec(memory_space=pltpu.SMEM)] + [vm] * len(xs) + [hb] * len(weights),
        out_specs=[vm] * n_out,
        scratch_shapes=[
            pltpu.VMEM((3, 16, 2, 64, width), jnp.bfloat16),
            pltpu.VMEM((rows, model), jnp.bfloat16),
            pltpu.VMEM((rows, width), jnp.float32),
            pltpu.VMEM((rows, width), jnp.float32),
            pltpu.VMEM((rows, width), jnp.bfloat16),
            pltpu.SemaphoreType.DMA((2, 16)),
            pltpu.SemaphoreType.DMA((2, 16)),
        ],
        compiler_params=pltpu.CompilerParams(vmem_limit_bytes=48 * 1024 * 1024),
        cost_estimate=pl.CostEstimate(
            flops=flops, bytes_accessed=6 * model * width, transcendentals=rows * width
        ),
        name="ffn_rows",
    )(coord, *xs, *weights)


def summed_decay(ld, scratch, span):
    scratch[...] = jnp.zeros_like(scratch)
    scratch[0:2, :] = ld[...]
    v = scratch[0:8, :]
    lane = lax.broadcasted_iota(jnp.int32, v.shape, 1) % span
    step = 1
    while step < span:
        v = v + jnp.where(lane >= step, pltpu.roll(v, step, 1), 0.0)
        step *= 2
    scratch[0:8, :] = v
    return v, scratch[...].T


def times_wide(q, state):
    high = state.astype(jnp.bfloat16)
    low = (state - high.astype(jnp.float32)).astype(jnp.bfloat16)
    return jnp.dot(q, high, preferred_element_type=jnp.float32) + jnp.dot(
        q, low, preferred_element_type=jnp.float32
    )


def state_body(ld, k, v, whole, message, first, scratch):
    rows, heads, depth = k.shape[0], ld.shape[0], first.shape[1]
    row, col = summed_decay(ld, scratch, BLOCK)
    scale = depth ** (-0.5)
    for h in range(heads):
        lanes = slice(h * depth, (h + 1) * depth)
        state = None
        total = 0.0
        for b in range(rows // BLOCK):
            here = slice(b * BLOCK, (b + 1) * BLOCK)
            last = row[h : h + 1, (b + 1) * BLOCK - 1 : (b + 1) * BLOCK]
            to_end = jnp.exp(last - col[here, h : h + 1]) * scale
            scaled = (k[here, lanes].astype(jnp.float32) * to_end).astype(jnp.bfloat16)
            added = lax.dot_general(
                scaled, v[here, lanes], (((0,), (0,)), ((), ())), preferred_element_type=jnp.float32
            )
            total = total + last
            if b == 0:
                first[h] = added
                state = added
            else:
                state = jnp.exp(last) * state + added
        decay = jnp.broadcast_to(jnp.exp(total), (1, depth))
        write_state(whole, h, decay, state)
        write_state(message, h, decay, state)


def within_body(ld, q, k, v, first, out, scratch):
    rows, heads, depth = q.shape[0], ld.shape[0], first.shape[1]
    row, col = summed_decay(ld, scratch, BLOCK)
    scale = depth ** (-0.5)
    tile = BLOCK // 2
    for h in range(heads):
        lanes = slice(h * depth, (h + 1) * depth)
        for b in range(rows // BLOCK):
            for i in range(2):
                t0 = b * BLOCK + i * tile
                seen = slice(b * BLOCK, t0 + tile)
                here = slice(t0, t0 + tile)
                span = (i + 1) * tile
                products = lax.dot_general(
                    q[here, lanes],
                    k[seen, lanes],
                    (((1,), (1,)), ((), ())),
                    preferred_element_type=jnp.float32,
                )
                gap = col[here, h : h + 1] - row[h : h + 1, seen]
                at = lax.broadcasted_iota(jnp.int32, (tile, span), 0) + i * tile
                causal = at >= lax.broadcasted_iota(jnp.int32, (tile, span), 1)
                weight = jnp.where(causal, jnp.exp(jnp.minimum(gap, 0.0)), 0.0)
                scores = (products * scale * weight).astype(jnp.bfloat16)
                result = jnp.dot(scores, v[seen, lanes], preferred_element_type=jnp.float32)
                if b > 0:
                    result = result + times_wide(q[here, lanes], first[h]) * jnp.exp(
                        col[here, h : h + 1]
                    )
                out[here, lanes] = result


def finish_body(coord, ld, q, within, gates, before, far3, far2, far1, gain, o0, o1, o2, o3, scratch, sums):
    rows, heads, depth = q.shape[0], ld.shape[0], before.shape[2]
    _, sums[...] = summed_decay(ld, scratch, rows)
    states = []
    for h in range(heads):
        state = read_state(far3, h)[1]
        for ref in (far2, far1):
            decay, more = read_state(ref, h)
            state = decay * state + more
        states.append(before[h, depth : depth + 1, :] * state + before[h, 0:depth, :])
    quarter = rows // RING
    for k, out in enumerate((o0, o1, o2, o3)):
        here = pl.ds(pl.multiple_of(((coord[3] + k) % RING) * quarter, quarter), quarter)
        for h in range(heads):
            lanes = slice(h * depth, (h + 1) * depth)
            retention = within[here, lanes] + times_wide(q[here, lanes], states[h]) * jnp.exp(
                sums[here, h : h + 1]
            )
            centered = retention - jnp.mean(retention, axis=-1, keepdims=True)
            variance = jnp.mean(centered * centered, axis=-1, keepdims=True)
            normed = centered * lax.rsqrt(variance + EPSILON) * gain[h : h + 1, :]
            g = gates[here, lanes].astype(jnp.float32)
            out[:, lanes] = (g * (1.0 / (1.0 + jnp.exp(-g))) * normed).astype(jnp.bfloat16)


def vmem_call(body, out_shape, *args, scratch=(), smem=0):
    vm = pl.BlockSpec(memory_space=pltpu.VMEM)
    return pl.pallas_call(
        body,
        out_shape=out_shape,
        in_specs=[pl.BlockSpec(memory_space=pltpu.SMEM)] * smem + [vm] * (len(args) - smem),
        out_specs=jax.tree.map(lambda _: vm, out_shape),
        scratch_shapes=list(scratch),
        compiler_params=pltpu.CompilerParams(vmem_limit_bytes=40 * 1024 * 1024),
    )(*args)


def mix_body(coord, r0, r1, r2, r3, own, near, near2, far, far2, resid, gain1, gain2, middle, out_a, out_b, acc):
    half = own.shape[0] // 2
    low = coord[2] == 0

    def part(cols, piece):
        return jnp.dot(cols, piece[...], preferred_element_type=jnp.float32)

    def rounded(v):
        return v.astype(jnp.bfloat16).astype(jnp.float32)

    def chosen(one, other):
        return jnp.where(low, one.astype(jnp.float32), other.astype(jnp.float32)).astype(jnp.bfloat16)

    left, right = r1[...], r3[...]
    far_a, far_b = r2[:, 0:half], r2[:, half:]
    acc[...] = rounded(part(r0[...], own))
    acc[...] += rounded(part(chosen(left, right), near))
    acc[...] += rounded(part(chosen(right, left), near2))
    far = part(chosen(far_a, far_b), far) + part(chosen(far_b, far_a), far2)
    mixed = rounded(acc[...] + rounded(far))
    mean = jnp.mean(mixed * mixed, axis=-1, keepdims=True)
    mid = resid[...].astype(jnp.float32) + mixed * lax.rsqrt(mean + EPSILON) * gain1[...]
    mid = mid.astype(jnp.bfloat16)
    middle[...] = mid
    mid = mid.astype(jnp.float32)
    mean = jnp.mean(mid * mid, axis=-1, keepdims=True)
    h = (mid * lax.rsqrt(mean + EPSILON) * gain2[...]).astype(jnp.bfloat16)
    out_a[...] = h[: h.shape[0] // 2]
    out_b[...] = h[h.shape[0] // 2 :]


def final_body(own_a, own_b, sum_a, sum_b, near_a, near_b, middle, gain, out):
    half = own_a.shape[0]
    for i, refs in enumerate(((own_a, sum_a, near_a), (own_b, sum_b, near_b))):
        here = slice(i * half, (i + 1) * half)
        total = sum(r[...].astype(jnp.float32) for r in refs)
        total = total.astype(jnp.bfloat16).astype(jnp.float32)
        mean = jnp.mean(total * total, axis=-1, keepdims=True)
        mid = middle[here, :].astype(jnp.float32)
        out[here, :] = (mid + total * lax.rsqrt(mean + EPSILON) * gain[...]).astype(jnp.bfloat16)


def read_state(ref, h):
    depth = ref.shape[2]
    state = ref[h, 0:depth, :].astype(jnp.float32)
    if ref.dtype == jnp.float32:
        return ref[h, depth : depth + 1, :], state
    tail = ref[h, depth : depth + 16, :].astype(jnp.float32)
    return tail[0:1] + tail[1:2], state


def write_state(ref, h, decay, state):
    depth = ref.shape[2]
    if ref.dtype == jnp.float32:
        ref[h, 0:depth, :] = state
        ref[h, depth : depth + 8, :] = jnp.broadcast_to(decay, (8, depth))
        return
    wide = jnp.broadcast_to(decay, (16, depth))
    high = wide.astype(jnp.bfloat16)
    low = (wide - high.astype(jnp.float32)).astype(jnp.bfloat16)
    at = lax.broadcasted_iota(jnp.int32, (16, depth), 0)
    ref[h, 0:depth, :] = state.astype(jnp.bfloat16)
    ref[h, depth : depth + 16, :] = jnp.where(at == 0, high, low)


def joined(earlier, later):
    return (earlier[0] * later[0], later[0] * earlier[1] + later[1])


def either(flag, one, other):
    return tuple(jnp.where(flag, a, b) for a, b in zip(one, other))


def pair_body(coord, total, got, new_total, before, message):
    upper = coord[2] == 1
    for h in range(total.shape[0]):
        mine, other = read_state(total, h), read_state(got, h)
        nothing = (jnp.ones_like(mine[0]), jnp.zeros_like(mine[1]))
        both = either(upper, joined(other, mine), joined(mine, other))
        write_state(new_total, h, *both)
        write_state(message, h, *both)
        write_state(before, h, *either(upper, other, nothing))


def plane_body(coord, total, inner, b1, b2, b3, before, message):
    y = coord[1]
    for h in range(total.shape[0]):
        mine = read_state(total, h)
        nothing = (jnp.ones_like(mine[0]), jnp.zeros_like(mine[1]))
        back = [read_state(r, h) for r in (b1, b2, b3)]
        past = nothing
        for k in (3, 2, 1):
            past = joined(past, either(y >= k, back[k - 1], nothing))
        whole = joined(past, mine)
        for k in (3, 2, 1):
            whole = joined(whole, either(y < k, back[k - 1], nothing))
        write_state(message, h, *whole)
        write_state(before, h, *joined(past, read_state(inner, h)))


def kernel(body, out_shape, *args, **more):
    return vmem_call(body, out_shape, *args, **more)


def shaped(dtype, *dims):
    return jax.ShapeDtypeStruct(dims, dtype)


def layer(
    queries,
    keys,
    values,
    gates,
    log_decay,
    norm_gain,
    out_weight,
    resid,
    post_mix_gain,
    pre_ffn_gain,
    w_gate,
    w_up,
    w_down,
    post_ffn_gain,
):
    f32, bf16 = jnp.float32, jnp.bfloat16
    z, y, c = (lax.axis_index(a) for a in SP)
    x = lax.axis_index("tp")
    coord = jnp.stack([z, y, c, x]).astype(jnp.int32)
    up1, down1 = along(1), along(-1)
    weights = gather_weights(w_gate, w_up, w_down)
    o_half = out_weight.shape[0] // 2
    turn = [(i, (i + 1) % RING) for i in range(RING)]
    turn += [(RING + i, RING + (i - 1) % RING) for i in range(RING)]
    o_near = lax.ppermute(out_weight, ("sp_2", "tp"), turn)
    o_fore = lax.dynamic_slice_in_dim(o_near, c * o_half, o_half, 0)
    o_far = lax.ppermute(o_fore, ("sp_2", "tp"), turn)
    o_near2 = lax.ppermute(o_near, "sp_2", flipped(2, 1))
    o_far2 = lax.ppermute(o_far, "sp_2", flipped(2, 1))

    rows, width = queries.shape
    heads = log_decay.shape[1]
    depth = width // heads
    ld = log_decay.T
    sums = pltpu.VMEM((128, rows), f32)
    total_shape = shaped(f32, heads, depth + 8, depth)
    message_shape = shaped(bf16, heads, depth + 16, depth)
    total, message, first = kernel(
        state_body,
        (total_shape, message_shape, shaped(f32, heads, depth, depth)),
        ld, keys, values,
        scratch=(sums,),
    )
    within = kernel(
        within_body, shaped(f32, rows, width), ld, queries, keys, values, first, scratch=(sums,)
    )
    got = lax.ppermute(message, "sp_2", flipped(2, 1))
    total, inner, message = kernel(
        pair_body, (total_shape, total_shape, message_shape), coord, total, got, smem=1
    )
    back = [lax.ppermute(message, "sp_1", along(k)) for k in (1, 2, 3)]
    before, message = kernel(
        plane_body, (total_shape, message_shape), coord, total, inner, *back, smem=1
    )
    back = [lax.ppermute(message, "sp_0", [(i, i + k) for i in range(RING - k)]) for k in (3, 2, 1)]
    quarter, model = resid.shape
    piece = shaped(bf16, quarter, width)
    turned = kernel(
        finish_body,
        (piece,) * RING,
        coord, ld, queries, within, gates, before, *back, norm_gain,
        scratch=(sums, pltpu.VMEM((rows, 128), f32)),
        smem=1,
    )
    turned = (turned[0], *(lax.ppermute(turned[k], "tp", along(k)) for k in (1, 2, 3)))
    half = quarter // 2
    middle, h_a, h_b = kernel(
        mix_body,
        (shaped(bf16, quarter, model), shaped(bf16, half, model), shaped(bf16, half, model)),
        coord, *turned, out_weight, o_near, o_near2, o_far, o_far2, resid,
        post_mix_gain.reshape(1, -1), pre_ffn_gain.reshape(1, -1),
        scratch=(pltpu.VMEM((quarter, model), f32),),
        smem=1,
    )

    r_a = lax.ppermute(h_a, "tp", up1)
    l_b = lax.ppermute(h_b, "tp", down1)
    far_a = lax.ppermute(r_a, "tp", up1)
    far_b = lax.ppermute(l_b, "tp", down1)
    r_b = lax.ppermute(h_b, "tp", up1)
    l_a = lax.ppermute(h_a, "tp", down1)

    def feed(*xs):
        return ffn(coord, weights, xs, 2)

    right_a, left_b = feed(r_a, l_b)
    opp_a, opp_b = feed(far_a, far_b)
    right_b, left_a = feed(r_b, l_a)
    own_a, own_b = feed(h_a, h_b)
    near_b = lax.ppermute(left_b, "tp", up1)
    near_a = lax.ppermute(right_a, "tp", down1)
    far_in_a = lax.ppermute(opp_a, "tp", up1)
    far_in_b = lax.ppermute(opp_b, "tp", down1)
    wide = lambda v: v.astype(f32)
    sum_a = lax.ppermute((wide(left_a) + wide(far_in_a)).astype(bf16), "tp", up1)
    sum_b = lax.ppermute((wide(right_b) + wide(far_in_b)).astype(bf16), "tp", down1)
    return kernel(
        final_body,
        shaped(bf16, quarter, model),
        own_a, own_b, sum_a, sum_b, near_a, near_b, middle, post_ffn_gain.reshape(1, -1),
    )


def solution(mesh):
    split = Mesh(mesh.devices.reshape(4, 4, 2, mesh.shape["tp"]), ("sp_0", "sp_1", "sp_2", "tp"))
    placed = (
        P(SP, "tp"),
        P(SP, "tp"),
        P(SP, "tp"),
        P(SP, "tp"),
        P(SP, "tp"),
        P("tp", None),
        P("tp", None),
        P(SP_TP, None),
        P(),
        P(),
        P(SP, "tp"),
        P(SP, "tp"),
        P("tp", SP),
        P(),
    )
    return jax.shard_map(
        layer, mesh=split, in_specs=placed, out_specs=P(SP_TP, None), check_vma=False
    )
```

```python
import functools

import jax
import jax.numpy as jnp
from jax import lax
from jax.experimental import pallas as pl
from jax.experimental.pallas import tpu as pltpu
from jax.sharding import Mesh
from jax.sharding import PartitionSpec as P


BLOCK = 512
SP = ("sp_0", "sp_1", "sp_2")
SP_TP = ("sp_0", "sp_1", "sp_2", "tp")
RING = 4
LIMIT = 16 * 1024 * 1024
EPSILON = 1e-06


def along(step):
    return [(i, (i + step) % RING) for i in range(RING)]


def role_shift(first, step):
    pairs = []
    for z in range(RING):
        for y in range(RING):
            for c in range(2):
                if (c == 0) == first:
                    to = (z, (y + step) % RING)
                else:
                    to = ((z + step) % RING, y)
                pairs.append((z * 8 + y * 2 + c, to[0] * 8 + to[1] * 2 + c))
    return pairs


def flipped(size, bit):
    return [(i, i ^ bit) for i in range(size)]


def gather_weights(w_gate, w_up, w_down):
    mine = jnp.stack([w_gate, w_up, w_down.T])
    near = functools.partial(role_shift, True)
    wide = functools.partial(role_shift, False)
    right = lax.ppermute(mine, SP, near(1))
    left = lax.ppermute(mine, SP, near(-1))
    far = lax.ppermute(mine, SP, near(2))
    s0 = jnp.stack([mine, right])
    s1 = jnp.stack([left, far])
    ra = lax.ppermute(s0, SP, wide(1))
    lb = lax.ppermute(s1, SP, wide(-1))
    fa = lax.ppermute(ra, SP, wide(1))
    fb = lax.ppermute(lb, SP, wide(-1))
    rb = lax.ppermute(s1, SP, wide(1))
    la = lax.ppermute(s0, SP, wide(-1))
    own = [s0, s1, ra, lb, fa, fb, rb, la]
    return own + [lax.ppermute(v, "sp_2", flipped(2, 1)) for v in own]


PIECES = ((0, 0), (2, 0), (0, 3), (2, 1), (0, 2), (2, 2), (2, 3), (0, 1))


def place_body(chosen, coord, *refs):
    count = 2 * len(chosen)
    pieces = refs[:count]
    w, sem = refs[-2:]
    z, y, c = coord[0], coord[1], coord[2]
    offs = (0, RING - 1, 1, 2)

    def copies(low):
        made = []
        for side in range(2):
            core = side if low else 1 - side
            for i, index in enumerate(chosen):
                first, away = PIECES[index]
                for k in range(2):
                    near = offs[first + k]
                    dz, dy = (away, near) if core == 0 else (near, away)
                    chip = ((z + dz) % RING) * RING + (y + dy) % RING
                    src = pieces[side * len(chosen) + i].at[k]
                    made.append(
                        pltpu.make_async_copy(src, w.at[:, chip, core], sem.at[len(made)])
                    )
        return made

    for low in (True, False):

        @pl.when((c == 0) == low)
        def _():
            made = copies(low)
            for one in made:
                one.start()
            for one in made:
                one.wait()


def place(coord, weights, chosen, w=None):
    n = len(PIECES)
    pieces = [weights[side * n + i] for side in range(2) for i in chosen]
    width = weights[0].shape[-1]
    hb = pl.BlockSpec(memory_space=pltpu.HBM)
    vm = pl.BlockSpec(memory_space=pltpu.VMEM)
    more = [] if w is None else [w]
    return pl.pallas_call(
        functools.partial(place_body, chosen),
        out_shape=jax.ShapeDtypeStruct((3, 16, 2, 64, width), jnp.bfloat16),
        in_specs=[pl.BlockSpec(memory_space=pltpu.SMEM)] + [hb] * len(pieces) + [vm] * len(more),
        out_specs=vm,
        scratch_shapes=[pltpu.SemaphoreType.DMA((2 * len(pieces),))],
        input_output_aliases={} if w is None else {1 + len(pieces): 0},
        compiler_params=pltpu.CompilerParams(vmem_limit_bytes=LIMIT),
    )(coord, *pieces, *more)


def ffn_body(n_in, n_out, *refs):
    xs = refs[:n_in]
    w = refs[n_in]
    outs = refs[n_in + 1 : n_in + 1 + n_out]
    x, both, hid = refs[n_in + 1 + n_out :]
    rows, model = x.shape
    width = both.shape[2]
    per = rows // n_in
    for i in range(n_in):
        x[i * per : (i + 1) * per, :] = xs[i][...]

    def enter(i, carry):
        both[i] = jnp.dot(x[...], w[i].reshape(model, width), preferred_element_type=jnp.float32)
        return carry

    lax.fori_loop(0, 2, enter, 0)
    g = both[0]
    hid[...] = (g * (1.0 / (1.0 + jnp.exp(-g))) * both[1]).astype(jnp.bfloat16)
    per_out = rows // n_out
    step = 256
    turns = 2

    def leave(turn, carry):
        for j in range(model // step // turns):
            k = turn * (model // step // turns) + j
            part = lax.dot_general(
                hid[...],
                w[2, pl.ds(2 * k, 2)].reshape(step, width),
                (((1,), (1,)), ((), ())),
                preferred_element_type=jnp.float32,
            ).astype(jnp.bfloat16)
            for i in range(n_out):
                outs[i][:, pl.ds(pl.multiple_of(k * step, step), step)] = part[
                    i * per_out : (i + 1) * per_out
                ]
        return carry

    lax.fori_loop(0, turns, leave, 0)


def ffn(w, xs, n_out):
    rows = sum(v.shape[0] for v in xs)
    model = xs[0].shape[1]
    width = w.shape[-1]
    vm = pl.BlockSpec(memory_space=pltpu.VMEM)
    return pl.pallas_call(
        functools.partial(ffn_body, len(xs), n_out),
        out_shape=[jax.ShapeDtypeStruct((rows // n_out, model), jnp.bfloat16)] * n_out,
        in_specs=[vm] * (len(xs) + 1),
        out_specs=[vm] * n_out,
        scratch_shapes=[
            pltpu.VMEM((rows, model), jnp.bfloat16),
            pltpu.VMEM((2, rows, width), jnp.float32),
            pltpu.VMEM((rows, width), jnp.bfloat16),
        ],
        compiler_params=pltpu.CompilerParams(vmem_limit_bytes=LIMIT),
        name="ffn_rows",
    )(*xs, w)


def summed_decay(ld, scratch, span):
    scratch[...] = jnp.zeros_like(scratch)
    scratch[0:2, :] = ld[...]
    v = scratch[0:8, :]
    lane = lax.broadcasted_iota(jnp.int32, v.shape, 1) % span
    step = 1
    while step < span:
        v = v + jnp.where(lane >= step, pltpu.roll(v, step, 1), 0.0)
        step *= 2
    scratch[0:8, :] = v
    return v, scratch[...].T


def times_wide(q, state):
    high = state.astype(jnp.bfloat16)
    low = (state - high.astype(jnp.float32)).astype(jnp.bfloat16)
    return jnp.dot(q, high, preferred_element_type=jnp.float32) + jnp.dot(
        q, low, preferred_element_type=jnp.float32
    )


def state_body(ld, k, v, whole, message, first, scratch):
    rows, heads, depth = k.shape[0], ld.shape[0], first.shape[1]
    row, col = summed_decay(ld, scratch, BLOCK)
    scale = depth ** (-0.5)
    for h in range(heads):
        lanes = slice(h * depth, (h + 1) * depth)
        state = None
        total = 0.0
        for b in range(rows // BLOCK):
            here = slice(b * BLOCK, (b + 1) * BLOCK)
            last = row[h : h + 1, (b + 1) * BLOCK - 1 : (b + 1) * BLOCK]
            to_end = jnp.exp(last - col[here, h : h + 1]) * scale
            scaled = (k[here, lanes].astype(jnp.float32) * to_end).astype(jnp.bfloat16)
            added = lax.dot_general(
                scaled, v[here, lanes], (((0,), (0,)), ((), ())), preferred_element_type=jnp.float32
            )
            total = total + last
            if b == 0:
                first[h] = added
                state = added
            else:
                state = jnp.exp(last) * state + added
        decay = jnp.broadcast_to(jnp.exp(total), (1, depth))
        write_state(whole, h, decay, state)
        write_state(message, h, decay, state)


def within_body(ld, q, k, v, first, out, scratch):
    rows, heads, depth = q.shape[0], ld.shape[0], first.shape[1]
    row, col = summed_decay(ld, scratch, BLOCK)
    scale = depth ** (-0.5)
    tile = BLOCK // 2
    for h in range(heads):
        lanes = slice(h * depth, (h + 1) * depth)
        for b in range(rows // BLOCK):
            for i in range(2):
                t0 = b * BLOCK + i * tile
                seen = slice(b * BLOCK, t0 + tile)
                here = slice(t0, t0 + tile)
                span = (i + 1) * tile
                products = lax.dot_general(
                    q[here, lanes],
                    k[seen, lanes],
                    (((1,), (1,)), ((), ())),
                    preferred_element_type=jnp.float32,
                )
                gap = col[here, h : h + 1] - row[h : h + 1, seen]
                at = lax.broadcasted_iota(jnp.int32, (tile, span), 0) + i * tile
                causal = at >= lax.broadcasted_iota(jnp.int32, (tile, span), 1)
                weight = jnp.where(causal, jnp.exp(jnp.minimum(gap, 0.0)), 0.0)
                scores = (products * scale * weight).astype(jnp.bfloat16)
                result = jnp.dot(scores, v[seen, lanes], preferred_element_type=jnp.float32)
                if b > 0:
                    result = result + times_wide(q[here, lanes], first[h]) * jnp.exp(
                        col[here, h : h + 1]
                    )
                out[here, lanes] = result


def finish_body(coord, ld, q, within, gates, before, far3, far2, far1, gain, o0, o1, o2, o3, scratch, sums):
    rows, heads, depth = q.shape[0], ld.shape[0], before.shape[2]
    _, sums[...] = summed_decay(ld, scratch, rows)
    states = []
    for h in range(heads):
        state = read_state(far3, h)[1]
        for ref in (far2, far1):
            decay, more = read_state(ref, h)
            state = decay * state + more
        states.append(before[h, depth : depth + 1, :] * state + before[h, 0:depth, :])
    quarter = rows // RING
    for k, out in enumerate((o0, o1, o2, o3)):
        here = pl.ds(pl.multiple_of(((coord[3] + k) % RING) * quarter, quarter), quarter)
        for h in range(heads):
            lanes = slice(h * depth, (h + 1) * depth)
            retention = within[here, lanes] + times_wide(q[here, lanes], states[h]) * jnp.exp(
                sums[here, h : h + 1]
            )
            centered = retention - jnp.mean(retention, axis=-1, keepdims=True)
            variance = jnp.mean(centered * centered, axis=-1, keepdims=True)
            normed = centered * lax.rsqrt(variance + EPSILON) * gain[h : h + 1, :]
            g = gates[here, lanes].astype(jnp.float32)
            out[:, lanes] = (g * (1.0 / (1.0 + jnp.exp(-g))) * normed).astype(jnp.bfloat16)


def vmem_call(body, out_shape, *args, scratch=(), smem=0):
    vm = pl.BlockSpec(memory_space=pltpu.VMEM)
    return pl.pallas_call(
        body,
        out_shape=out_shape,
        in_specs=[pl.BlockSpec(memory_space=pltpu.SMEM)] * smem + [vm] * (len(args) - smem),
        out_specs=jax.tree.map(lambda _: vm, out_shape),
        scratch_shapes=list(scratch),
        compiler_params=pltpu.CompilerParams(vmem_limit_bytes=LIMIT),
    )(*args)


def mix_body(coord, r0, r1, r2, r3, own, near, near2, far, far2, resid, gain1, gain2, middle, out_a, out_b, acc):
    half = own.shape[0] // 2
    low = coord[2] == 0

    def part(cols, piece):
        return jnp.dot(cols, piece[...], preferred_element_type=jnp.float32)

    def rounded(v):
        return v.astype(jnp.bfloat16).astype(jnp.float32)

    def chosen(one, other):
        return jnp.where(low, one.astype(jnp.float32), other.astype(jnp.float32)).astype(jnp.bfloat16)

    left, right = r1[...], r3[...]
    far_a, far_b = r2[:, 0:half], r2[:, half:]
    acc[...] = rounded(part(r0[...], own))
    acc[...] += rounded(part(chosen(left, right), near))
    acc[...] += rounded(part(chosen(right, left), near2))
    far = part(chosen(far_a, far_b), far) + part(chosen(far_b, far_a), far2)
    mixed = rounded(acc[...] + rounded(far))
    mean = jnp.mean(mixed * mixed, axis=-1, keepdims=True)
    mid = resid[...].astype(jnp.float32) + mixed * lax.rsqrt(mean + EPSILON) * gain1[...]
    mid = mid.astype(jnp.bfloat16)
    middle[...] = mid
    mid = mid.astype(jnp.float32)
    mean = jnp.mean(mid * mid, axis=-1, keepdims=True)
    h = (mid * lax.rsqrt(mean + EPSILON) * gain2[...]).astype(jnp.bfloat16)
    out_a[...] = h[: h.shape[0] // 2]
    out_b[...] = h[h.shape[0] // 2 :]


def final_body(own_a, own_b, sum_a, sum_b, near_a, near_b, middle, gain, out):
    half = own_a.shape[0]
    for i, refs in enumerate(((own_a, sum_a, near_a), (own_b, sum_b, near_b))):
        here = slice(i * half, (i + 1) * half)
        total = sum(r[...].astype(jnp.float32) for r in refs)
        total = total.astype(jnp.bfloat16).astype(jnp.float32)
        mean = jnp.mean(total * total, axis=-1, keepdims=True)
        mid = middle[here, :].astype(jnp.float32)
        out[here, :] = (mid + total * lax.rsqrt(mean + EPSILON) * gain[...]).astype(jnp.bfloat16)


def read_state(ref, h):
    depth = ref.shape[2]
    state = ref[h, 0:depth, :].astype(jnp.float32)
    if ref.dtype == jnp.float32:
        return ref[h, depth : depth + 1, :], state
    tail = ref[h, depth : depth + 16, :].astype(jnp.float32)
    return tail[0:1] + tail[1:2], state


def write_state(ref, h, decay, state):
    depth = ref.shape[2]
    if ref.dtype == jnp.float32:
        ref[h, 0:depth, :] = state
        ref[h, depth : depth + 8, :] = jnp.broadcast_to(decay, (8, depth))
        return
    wide = jnp.broadcast_to(decay, (16, depth))
    high = wide.astype(jnp.bfloat16)
    low = (wide - high.astype(jnp.float32)).astype(jnp.bfloat16)
    at = lax.broadcasted_iota(jnp.int32, (16, depth), 0)
    ref[h, 0:depth, :] = state.astype(jnp.bfloat16)
    ref[h, depth : depth + 16, :] = jnp.where(at == 0, high, low)


def joined(earlier, later):
    return (earlier[0] * later[0], later[0] * earlier[1] + later[1])


def either(flag, one, other):
    return tuple(jnp.where(flag, a, b) for a, b in zip(one, other))


def pair_body(coord, total, got, new_total, before, message):
    upper = coord[2] == 1
    for h in range(total.shape[0]):
        mine, other = read_state(total, h), read_state(got, h)
        nothing = (jnp.ones_like(mine[0]), jnp.zeros_like(mine[1]))
        both = either(upper, joined(other, mine), joined(mine, other))
        write_state(new_total, h, *both)
        write_state(message, h, *both)
        write_state(before, h, *either(upper, other, nothing))


def plane_body(coord, total, inner, b1, b2, b3, before, message):
    y = coord[1]
    for h in range(total.shape[0]):
        mine = read_state(total, h)
        nothing = (jnp.ones_like(mine[0]), jnp.zeros_like(mine[1]))
        back = [read_state(r, h) for r in (b1, b2, b3)]
        past = nothing
        for k in (3, 2, 1):
            past = joined(past, either(y >= k, back[k - 1], nothing))
        whole = joined(past, mine)
        for k in (3, 2, 1):
            whole = joined(whole, either(y < k, back[k - 1], nothing))
        write_state(message, h, *whole)
        write_state(before, h, *joined(past, read_state(inner, h)))


def kernel(body, out_shape, *args, **more):
    return vmem_call(body, out_shape, *args, **more)


def shaped(dtype, *dims):
    return jax.ShapeDtypeStruct(dims, dtype)


def layer(
    queries,
    keys,
    values,
    gates,
    log_decay,
    norm_gain,
    out_weight,
    resid,
    post_mix_gain,
    pre_ffn_gain,
    w_gate,
    w_up,
    w_down,
    post_ffn_gain,
):
    f32, bf16 = jnp.float32, jnp.bfloat16
    z, y, c = (lax.axis_index(a) for a in SP)
    x = lax.axis_index("tp")
    coord = jnp.stack([z, y, c, x]).astype(jnp.int32)
    up1, down1 = along(1), along(-1)
    weights = gather_weights(w_gate, w_up, w_down)
    o_half = out_weight.shape[0] // 2
    turn = [(i, (i + 1) % RING) for i in range(RING)]
    turn += [(RING + i, RING + (i - 1) % RING) for i in range(RING)]
    o_near = lax.ppermute(out_weight, ("sp_2", "tp"), turn)
    o_fore = lax.dynamic_slice_in_dim(o_near, c * o_half, o_half, 0)
    o_far = lax.ppermute(o_fore, ("sp_2", "tp"), turn)
    o_near2 = lax.ppermute(o_near, "sp_2", flipped(2, 1))
    o_far2 = lax.ppermute(o_far, "sp_2", flipped(2, 1))

    rows, width = queries.shape
    heads = log_decay.shape[1]
    depth = width // heads
    ld = log_decay.T
    sums = pltpu.VMEM((128, rows), f32)
    total_shape = shaped(f32, heads, depth + 8, depth)
    message_shape = shaped(bf16, heads, depth + 16, depth)
    total, message, first = kernel(
        state_body,
        (total_shape, message_shape, shaped(f32, heads, depth, depth)),
        ld, keys, values,
        scratch=(sums,),
    )
    within = kernel(
        within_body, shaped(f32, rows, width), ld, queries, keys, values, first, scratch=(sums,)
    )
    got = lax.ppermute(message, "sp_2", flipped(2, 1))
    total, inner, message = kernel(
        pair_body, (total_shape, total_shape, message_shape), coord, total, got, smem=1
    )
    back = [lax.ppermute(message, "sp_1", along(k)) for k in (1, 2, 3)]
    before, message = kernel(
        plane_body, (total_shape, message_shape), coord, total, inner, *back, smem=1
    )
    back = [lax.ppermute(message, "sp_0", [(i, i + k) for i in range(RING - k)]) for k in (3, 2, 1)]
    quarter, model = resid.shape
    piece = shaped(bf16, quarter, width)
    turned = kernel(
        finish_body,
        (piece,) * RING,
        coord, ld, queries, within, gates, before, *back, norm_gain,
        scratch=(sums, pltpu.VMEM((rows, 128), f32)),
        smem=1,
    )
    turned = (turned[0], *(lax.ppermute(turned[k], "tp", along(k)) for k in (1, 2, 3)))
    half = quarter // 2
    middle, h_a, h_b = kernel(
        mix_body,
        (shaped(bf16, quarter, model), shaped(bf16, half, model), shaped(bf16, half, model)),
        coord, *turned, out_weight, o_near, o_near2, o_far, o_far2, resid,
        post_mix_gain.reshape(1, -1), pre_ffn_gain.reshape(1, -1),
        scratch=(pltpu.VMEM((quarter, model), f32),),
        smem=1,
    )

    r_a = lax.ppermute(h_a, "tp", up1)
    l_b = lax.ppermute(h_b, "tp", down1)
    far_a = lax.ppermute(r_a, "tp", up1)
    far_b = lax.ppermute(l_b, "tp", down1)
    r_b = lax.ppermute(h_b, "tp", up1)
    l_a = lax.ppermute(h_a, "tp", down1)

    w = place(coord, weights, (0, 1, 2, 3, 6, 7))
    w = place(coord, weights, (4, 5), w)

    def feed(*xs):
        return ffn(w, xs, 2)

    right_a, left_b = feed(r_a, l_b)
    opp_a, opp_b = feed(far_a, far_b)
    right_b, left_a = feed(r_b, l_a)
    own_a, own_b = feed(h_a, h_b)
    near_b = lax.ppermute(left_b, "tp", up1)
    near_a = lax.ppermute(right_a, "tp", down1)
    far_in_a = lax.ppermute(opp_a, "tp", up1)
    far_in_b = lax.ppermute(opp_b, "tp", down1)
    wide = lambda v: v.astype(f32)
    sum_a = lax.ppermute((wide(left_a) + wide(far_in_a)).astype(bf16), "tp", up1)
    sum_b = lax.ppermute((wide(right_b) + wide(far_in_b)).astype(bf16), "tp", down1)
    return kernel(
        final_body,
        shaped(bf16, quarter, model),
        own_a, own_b, sum_a, sum_b, near_a, near_b, middle, post_ffn_gain.reshape(1, -1),
    )


def solution(mesh):
    split = Mesh(mesh.devices.reshape(4, 4, 2, mesh.shape["tp"]), ("sp_0", "sp_1", "sp_2", "tp"))
    placed = (
        P(SP, "tp"),
        P(SP, "tp"),
        P(SP, "tp"),
        P(SP, "tp"),
        P(SP, "tp"),
        P("tp", None),
        P("tp", None),
        P(SP_TP, None),
        P(),
        P(),
        P(SP, "tp"),
        P(SP, "tp"),
        P("tp", SP),
        P(),
    )
    return jax.shard_map(
        layer, mesh=split, in_specs=placed, out_specs=P(SP_TP, None), check_vma=False
    )
```

```python
import functools

import jax
import jax.numpy as jnp
from jax import lax
from jax.experimental import pallas as pl
from jax.experimental.pallas import tpu as pltpu
from jax.sharding import Mesh
from jax.sharding import PartitionSpec as P


BLOCK = 512
SP = ("sp_0", "sp_1", "sp_2")
SP_TP = ("sp_0", "sp_1", "sp_2", "tp")
RING = 4
LIMIT = 16 * 1024 * 1024
EPSILON = 1e-06


def along(step):
    return [(i, (i + step) % RING) for i in range(RING)]


def role_shift(first, step):
    pairs = []
    for z in range(RING):
        for y in range(RING):
            for c in range(2):
                if (c == 0) == first:
                    to = (z, (y + step) % RING)
                else:
                    to = ((z + step) % RING, y)
                pairs.append((z * 8 + y * 2 + c, to[0] * 8 + to[1] * 2 + c))
    return pairs


def flipped(size, bit):
    return [(i, i ^ bit) for i in range(size)]


def near_shards(mine):
    near = functools.partial(role_shift, True)
    return (
        lax.ppermute(mine, SP, near(1)),
        lax.ppermute(mine, SP, near(-1)),
        lax.ppermute(mine, SP, near(2)),
    )


def far_shards(s0, s1):
    wide = functools.partial(role_shift, False)
    ra = lax.ppermute(s0, SP, wide(1))
    lb = lax.ppermute(s1, SP, wide(-1))
    fa = lax.ppermute(ra, SP, wide(1))
    fb = lax.ppermute(lb, SP, wide(-1))
    rb = lax.ppermute(s1, SP, wide(1))
    la = lax.ppermute(s0, SP, wide(-1))
    own = [s0, s1, ra, lb, fa, fb, rb, la]
    return own + [lax.ppermute(v, "sp_2", flipped(2, 1)) for v in own]


PIECES = ((0, 0), (2, 0), (0, 3), (2, 1), (0, 2), (2, 2), (2, 3), (0, 1))


def place_body(chosen, coord, *refs):
    count = 2 * len(chosen)
    pieces = refs[:count]
    w, sem = refs[-2:]
    z, y, c = coord[0], coord[1], coord[2]
    offs = (0, RING - 1, 1, 2)

    def copies(low):
        made = []
        for side in range(2):
            core = side if low else 1 - side
            for i, index in enumerate(chosen):
                first, away = PIECES[index]
                for k in range(2):
                    near = offs[first + k]
                    dz, dy = (away, near) if core == 0 else (near, away)
                    chip = ((z + dz) % RING) * RING + (y + dy) % RING
                    src = pieces[side * len(chosen) + i].at[k]
                    made.append(
                        pltpu.make_async_copy(src, w.at[:, chip, core], sem.at[len(made)])
                    )
        return made

    for low in (True, False):

        @pl.when((c == 0) == low)
        def _():
            made = copies(low)
            for one in made:
                one.start()
            for one in made:
                one.wait()


def place(coord, weights, chosen, w=None):
    n = len(PIECES)
    pieces = [weights[side * n + i] for side in range(2) for i in chosen]
    width = weights[0].shape[-1]
    hb = pl.BlockSpec(memory_space=pltpu.HBM)
    vm = pl.BlockSpec(memory_space=pltpu.VMEM)
    more = [] if w is None else [w]
    return pl.pallas_call(
        functools.partial(place_body, chosen),
        out_shape=jax.ShapeDtypeStruct((3, 16, 2, 64, width), jnp.bfloat16),
        in_specs=[pl.BlockSpec(memory_space=pltpu.SMEM)] + [hb] * len(pieces) + [vm] * len(more),
        out_specs=vm,
        scratch_shapes=[pltpu.SemaphoreType.DMA((2 * len(pieces),))],
        input_output_aliases={} if w is None else {1 + len(pieces): 0},
        compiler_params=pltpu.CompilerParams(vmem_limit_bytes=LIMIT),
    )(coord, *pieces, *more)


def ffn_body(n_in, n_out, *refs):
    xs = refs[:n_in]
    w = refs[n_in]
    outs = refs[n_in + 1 : n_in + 1 + n_out]
    x, both, hid = refs[n_in + 1 + n_out :]
    rows, model = x.shape
    width = both.shape[2]
    per = rows // n_in
    for i in range(n_in):
        x[i * per : (i + 1) * per, :] = xs[i][...]

    def enter(i, carry):
        both[i] = jnp.dot(x[...], w[i].reshape(model, width), preferred_element_type=jnp.float32)
        return carry

    lax.fori_loop(0, 2, enter, 0)
    g = both[0]
    hid[...] = (g * (1.0 / (1.0 + jnp.exp(-g))) * both[1]).astype(jnp.bfloat16)
    per_out = rows // n_out
    step = 256
    turns = 2

    def leave(turn, carry):
        for j in range(model // step // turns):
            k = turn * (model // step // turns) + j
            part = lax.dot_general(
                hid[...],
                w[2, pl.ds(2 * k, 2)].reshape(step, width),
                (((1,), (1,)), ((), ())),
                preferred_element_type=jnp.float32,
            ).astype(jnp.bfloat16)
            for i in range(n_out):
                outs[i][:, pl.ds(pl.multiple_of(k * step, step), step)] = part[
                    i * per_out : (i + 1) * per_out
                ]
        return carry

    lax.fori_loop(0, turns, leave, 0)


def ffn(w, xs, n_out):
    rows = sum(v.shape[0] for v in xs)
    model = xs[0].shape[1]
    width = w.shape[-1]
    vm = pl.BlockSpec(memory_space=pltpu.VMEM)
    return pl.pallas_call(
        functools.partial(ffn_body, len(xs), n_out),
        out_shape=[jax.ShapeDtypeStruct((rows // n_out, model), jnp.bfloat16)] * n_out,
        in_specs=[vm] * (len(xs) + 1),
        out_specs=[vm] * n_out,
        scratch_shapes=[
            pltpu.VMEM((rows, model), jnp.bfloat16),
            pltpu.VMEM((2, rows, width), jnp.float32),
            pltpu.VMEM((rows, width), jnp.bfloat16),
        ],
        compiler_params=pltpu.CompilerParams(vmem_limit_bytes=LIMIT),
        name="ffn_rows",
    )(*xs, w)


def summed_decay(ld, scratch, span):
    scratch[...] = jnp.zeros_like(scratch)
    scratch[0:2, :] = ld[...]
    v = scratch[0:8, :]
    lane = lax.broadcasted_iota(jnp.int32, v.shape, 1) % span
    step = 1
    while step < span:
        v = v + jnp.where(lane >= step, pltpu.roll(v, step, 1), 0.0)
        step *= 2
    scratch[0:8, :] = v
    return v, scratch[...].T


def times_wide(q, state):
    high = state.astype(jnp.bfloat16)
    low = (state - high.astype(jnp.float32)).astype(jnp.bfloat16)
    return jnp.dot(q, high, preferred_element_type=jnp.float32) + jnp.dot(
        q, low, preferred_element_type=jnp.float32
    )


def block_state(row, col, k, v, h, b, depth):
    lanes = slice(h * depth, (h + 1) * depth)
    here = slice(b * BLOCK, (b + 1) * BLOCK)
    last = row[h : h + 1, (b + 1) * BLOCK - 1 : (b + 1) * BLOCK]
    to_end = jnp.exp(last - col[here, h : h + 1]) * depth ** (-0.5)
    scaled = (k[here, lanes].astype(jnp.float32) * to_end).astype(jnp.bfloat16)
    added = lax.dot_general(
        scaled, v[here, lanes], (((0,), (0,)), ((), ())), preferred_element_type=jnp.float32
    )
    return added, last


def state_body(ld, k, v, message, scratch):
    rows, heads, depth = k.shape[0], ld.shape[0], message.shape[2]
    row, col = summed_decay(ld, scratch, BLOCK)
    for h in range(heads):
        state, total = block_state(row, col, k, v, h, 0, depth)
        for b in range(1, rows // BLOCK):
            added, last = block_state(row, col, k, v, h, b, depth)
            state = jnp.exp(last) * state + added
            total = total + last
        write_state(message, h, jnp.broadcast_to(jnp.exp(total), (1, depth)), state)


def joining(one, other, out, sem):
    made = [pltpu.make_async_copy(r, out.at[i], sem.at[i]) for i, r in enumerate((one, other))]
    for copy in made:
        copy.start()
    return made


def within_body(ld, q, k, v, near, far, out, both, scratch, sem):
    rows, heads = q.shape[0], ld.shape[0]
    depth = q.shape[1] // heads
    copies = joining(near, far, both, sem)
    row, col = summed_decay(ld, scratch, BLOCK)
    scale = depth ** (-0.5)
    tile = BLOCK // 2
    for h in range(heads):
        lanes = slice(h * depth, (h + 1) * depth)
        state = None
        for b in range(rows // BLOCK):
            for i in range(2):
                t0 = b * BLOCK + i * tile
                seen = slice(b * BLOCK, t0 + tile)
                here = slice(t0, t0 + tile)
                span = (i + 1) * tile
                products = lax.dot_general(
                    q[here, lanes],
                    k[seen, lanes],
                    (((1,), (1,)), ((), ())),
                    preferred_element_type=jnp.float32,
                )
                gap = col[here, h : h + 1] - row[h : h + 1, seen]
                at = lax.broadcasted_iota(jnp.int32, (tile, span), 0) + i * tile
                causal = at >= lax.broadcasted_iota(jnp.int32, (tile, span), 1)
                weight = jnp.where(causal, jnp.exp(jnp.minimum(gap, 0.0)), 0.0)
                scores = (products * scale * weight).astype(jnp.bfloat16)
                result = jnp.dot(scores, v[seen, lanes], preferred_element_type=jnp.float32)
                if b > 0:
                    result = result + times_wide(q[here, lanes], state) * jnp.exp(
                        col[here, h : h + 1]
                    )
                out[here, lanes] = result
            if b + 1 < rows // BLOCK:
                added, last = block_state(row, col, k, v, h, b, depth)
                state = added if b == 0 else jnp.exp(last) * state + added
    for copy in copies:
        copy.wait()


def finish_body(coord, ld, q, within, gates, before, far3, far2, far1, gain, w_near, w_far, o0, o1, o2, o3, both, scratch, sums, sem):
    rows, heads, depth = q.shape[0], ld.shape[0], before.shape[2]
    copies = joining(w_near, w_far, both, sem)
    _, sums[...] = summed_decay(ld, scratch, rows)
    states = []
    for h in range(heads):
        state = read_state(far3, h)[1]
        for ref in (far2, far1):
            decay, more = read_state(ref, h)
            state = decay * state + more
        states.append(before[h, depth : depth + 1, :] * state + before[h, 0:depth, :])
    quarter = rows // RING
    for k, out in enumerate((o0, o1, o2, o3)):
        here = pl.ds(pl.multiple_of(((coord[3] + k) % RING) * quarter, quarter), quarter)
        for h in range(heads):
            lanes = slice(h * depth, (h + 1) * depth)
            retention = within[here, lanes] + times_wide(q[here, lanes], states[h]) * jnp.exp(
                sums[here, h : h + 1]
            )
            centered = retention - jnp.mean(retention, axis=-1, keepdims=True)
            variance = jnp.mean(centered * centered, axis=-1, keepdims=True)
            normed = centered * lax.rsqrt(variance + EPSILON) * gain[h : h + 1, :]
            g = gates[here, lanes].astype(jnp.float32)
            out[:, lanes] = (g * (1.0 / (1.0 + jnp.exp(-g))) * normed).astype(jnp.bfloat16)
    for copy in copies:
        copy.wait()


def vmem_call(body, out_shape, *args, scratch=(), smem=0, hbm=(), hbm_out=()):
    vm = pl.BlockSpec(memory_space=pltpu.VMEM)
    hb = pl.BlockSpec(memory_space=pltpu.HBM)
    sm = pl.BlockSpec(memory_space=pltpu.SMEM)
    specs = [sm if i < smem else hb if i in hbm else vm for i in range(len(args))]
    if isinstance(out_shape, tuple):
        out_specs = tuple(hb if i in hbm_out else vm for i in range(len(out_shape)))
    else:
        out_specs = vm
    return pl.pallas_call(
        body,
        out_shape=out_shape,
        in_specs=specs,
        out_specs=out_specs,
        scratch_shapes=list(scratch),
        compiler_params=pltpu.CompilerParams(vmem_limit_bytes=LIMIT),
    )(*args)


def mix_body(coord, r0, r1, r2, r3, own, near, near2, far, far2, resid, gain1, gain2, middle, out_a, out_b):
    half = own.shape[0] // 2
    low = coord[2] == 0

    def chosen(one, other):
        return jnp.where(low, one.astype(jnp.float32), other.astype(jnp.float32)).astype(jnp.bfloat16)

    left, right = r1[...], r3[...]
    far_a, far_b = r2[:, 0:half], r2[:, half:]
    columns = [
        r0[...],
        chosen(left, right),
        chosen(right, left),
        chosen(far_a, far_b),
        chosen(far_b, far_a),
    ]
    rows = [v[...] for v in (own, near, near2, far, far2)]
    mixed = jnp.dot(
        jnp.concatenate(columns, axis=1),
        jnp.concatenate(rows, axis=0),
        preferred_element_type=jnp.float32,
    )
    mixed = mixed.astype(jnp.bfloat16).astype(jnp.float32)
    mean = jnp.mean(mixed * mixed, axis=-1, keepdims=True)
    mid = resid[...].astype(jnp.float32) + mixed * lax.rsqrt(mean + EPSILON) * gain1[...]
    mid = mid.astype(jnp.bfloat16)
    middle[...] = mid
    mid = mid.astype(jnp.float32)
    mean = jnp.mean(mid * mid, axis=-1, keepdims=True)
    h = (mid * lax.rsqrt(mean + EPSILON) * gain2[...]).astype(jnp.bfloat16)
    out_a[...] = h[: h.shape[0] // 2]
    out_b[...] = h[h.shape[0] // 2 :]


def final_body(own_a, own_b, sum_a, sum_b, near_a, near_b, middle, gain, out):
    half = own_a.shape[0]
    for i, refs in enumerate(((own_a, sum_a, near_a), (own_b, sum_b, near_b))):
        here = slice(i * half, (i + 1) * half)
        total = sum(r[...].astype(jnp.float32) for r in refs)
        total = total.astype(jnp.bfloat16).astype(jnp.float32)
        mean = jnp.mean(total * total, axis=-1, keepdims=True)
        mid = middle[here, :].astype(jnp.float32)
        out[here, :] = (mid + total * lax.rsqrt(mean + EPSILON) * gain[...]).astype(jnp.bfloat16)


def read_state(ref, h):
    depth = ref.shape[2]
    state = ref[h, 0:depth, :].astype(jnp.float32)
    if ref.dtype == jnp.float32:
        return ref[h, depth : depth + 1, :], state
    tail = ref[h, depth : depth + 16, :].astype(jnp.float32)
    return tail[0:1] + tail[1:2], state


def write_state(ref, h, decay, state):
    depth = ref.shape[2]
    if ref.dtype == jnp.float32:
        ref[h, 0:depth, :] = state
        ref[h, depth : depth + 8, :] = jnp.broadcast_to(decay, (8, depth))
        return
    wide = jnp.broadcast_to(decay, (16, depth))
    high = wide.astype(jnp.bfloat16)
    low = (wide - high.astype(jnp.float32)).astype(jnp.bfloat16)
    at = lax.broadcasted_iota(jnp.int32, (16, depth), 0)
    ref[h, 0:depth, :] = state.astype(jnp.bfloat16)
    ref[h, depth : depth + 16, :] = jnp.where(at == 0, high, low)


def joined(earlier, later):
    return (earlier[0] * later[0], later[0] * earlier[1] + later[1])


def either(flag, one, other):
    return tuple(jnp.where(flag, a, b) for a, b in zip(one, other))


def pair_body(coord, own, got, before, message):
    upper = coord[2] == 1
    for h in range(own.shape[0]):
        mine, other = read_state(own, h), read_state(got, h)
        nothing = (jnp.ones_like(mine[0]), jnp.zeros_like(mine[1]))
        both = either(upper, joined(other, mine), joined(mine, other))
        write_state(message, h, *both)
        write_state(before, h, *either(upper, other, nothing))


def plane_body(coord, own, inner, b1, b2, b3, before, message):
    y = coord[1]
    for h in range(own.shape[0]):
        mine = read_state(own, h)
        nothing = (jnp.ones_like(mine[0]), jnp.zeros_like(mine[1]))
        back = [read_state(r, h) for r in (b1, b2, b3)]
        past = nothing
        for k in (3, 2, 1):
            past = joined(past, either(y >= k, back[k - 1], nothing))
        whole = joined(past, mine)
        for k in (3, 2, 1):
            whole = joined(whole, either(y < k, back[k - 1], nothing))
        write_state(message, h, *whole)
        write_state(before, h, *joined(past, read_state(inner, h)))


def kernel(body, out_shape, *args, **more):
    return vmem_call(body, out_shape, *args, **more)


def shaped(dtype, *dims):
    return jax.ShapeDtypeStruct(dims, dtype)


def layer(
    queries,
    keys,
    values,
    gates,
    log_decay,
    norm_gain,
    out_weight,
    resid,
    post_mix_gain,
    pre_ffn_gain,
    w_gate,
    w_up,
    w_down,
    post_ffn_gain,
):
    f32, bf16 = jnp.float32, jnp.bfloat16
    z, y, c = (lax.axis_index(a) for a in SP)
    x = lax.axis_index("tp")
    coord = jnp.stack([z, y, c, x]).astype(jnp.int32)
    up1, down1 = along(1), along(-1)
    o_half = out_weight.shape[0] // 2
    turn = [(i, (i + 1) % RING) for i in range(RING)]
    turn += [(RING + i, RING + (i - 1) % RING) for i in range(RING)]
    o_near = lax.ppermute(out_weight, ("sp_2", "tp"), turn)
    o_fore = lax.dynamic_slice_in_dim(o_near, c * o_half, o_half, 0)
    o_far = lax.ppermute(o_fore, ("sp_2", "tp"), turn)
    o_near2 = lax.ppermute(o_near, "sp_2", flipped(2, 1))
    o_far2 = lax.ppermute(o_far, "sp_2", flipped(2, 1))

    rows, width = queries.shape
    heads = log_decay.shape[1]
    depth = width // heads
    ld = log_decay.T
    sums = pltpu.VMEM((128, rows), f32)
    total_shape = shaped(f32, heads, depth + 8, depth)
    message_shape = shaped(bf16, heads, depth + 16, depth)
    block = w_gate.shape
    mine = jnp.stack([w_gate, w_up, w_down.T])
    message = kernel(state_body, message_shape, ld, keys, values, scratch=(sums,))
    w_right, w_left, w_far = near_shards(mine)
    pair = pltpu.SemaphoreType.DMA((2,))
    within, s0 = kernel(
        within_body,
        (shaped(f32, rows, width), shaped(bf16, 2, 3, *block)),
        ld, queries, keys, values, mine, w_right,
        scratch=(sums, pair),
        hbm=(4, 5),
        hbm_out=(1,),
    )
    got = lax.ppermute(message, "sp_2", flipped(2, 1))
    inner, message = kernel(pair_body, (total_shape, message_shape), coord, message, got, smem=1)
    back = [lax.ppermute(message, "sp_1", along(k)) for k in (1, 2, 3)]
    before, message = kernel(
        plane_body, (total_shape, message_shape), coord, message, inner, *back, smem=1
    )
    back = [lax.ppermute(message, "sp_0", [(i, i + k) for i in range(RING - k)]) for k in (3, 2, 1)]
    quarter, model = resid.shape
    piece = shaped(bf16, quarter, width)
    *turned, s1 = kernel(
        finish_body,
        (piece,) * RING + (shaped(bf16, 2, 3, *block),),
        coord, ld, queries, within, gates, before, *back, norm_gain, w_left, w_far,
        scratch=(sums, pltpu.VMEM((rows, 128), f32), pair),
        smem=1,
        hbm=(10, 11),
        hbm_out=(4,),
    )
    weights = far_shards(s0, s1)
    turned = (turned[0], *(lax.ppermute(turned[k], "tp", along(k)) for k in (1, 2, 3)))
    half = quarter // 2
    middle, h_a, h_b = kernel(
        mix_body,
        (shaped(bf16, quarter, model), shaped(bf16, half, model), shaped(bf16, half, model)),
        coord, *turned, out_weight, o_near, o_near2, o_far, o_far2, resid,
        post_mix_gain.reshape(1, -1), pre_ffn_gain.reshape(1, -1),
        smem=1,
    )

    r_a = lax.ppermute(h_a, "tp", up1)
    l_b = lax.ppermute(h_b, "tp", down1)
    far_a = lax.ppermute(r_a, "tp", up1)
    far_b = lax.ppermute(l_b, "tp", down1)
    r_b = lax.ppermute(h_b, "tp", up1)
    l_a = lax.ppermute(h_a, "tp", down1)

    w = place(coord, weights, (0, 1, 2, 3, 6, 7))
    w = place(coord, weights, (4, 5), w)

    def feed(*xs):
        return ffn(w, xs, 2)

    right_a, left_b = feed(r_a, l_b)
    opp_a, opp_b = feed(far_a, far_b)
    right_b, left_a = feed(r_b, l_a)
    own_a, own_b = feed(h_a, h_b)
    near_b = lax.ppermute(left_b, "tp", up1)
    near_a = lax.ppermute(right_a, "tp", down1)
    far_in_a = lax.ppermute(opp_a, "tp", up1)
    far_in_b = lax.ppermute(opp_b, "tp", down1)
    wide = lambda v: v.astype(f32)
    sum_a = lax.ppermute((wide(left_a) + wide(far_in_a)).astype(bf16), "tp", up1)
    sum_b = lax.ppermute((wide(right_b) + wide(far_in_b)).astype(bf16), "tp", down1)
    return kernel(
        final_body,
        shaped(bf16, quarter, model),
        own_a, own_b, sum_a, sum_b, near_a, near_b, middle, post_ffn_gain.reshape(1, -1),
    )


def solution(mesh):
    split = Mesh(mesh.devices.reshape(4, 4, 2, mesh.shape["tp"]), ("sp_0", "sp_1", "sp_2", "tp"))
    placed = (
        P(SP, "tp"),
        P(SP, "tp"),
        P(SP, "tp"),
        P(SP, "tp"),
        P(SP, "tp"),
        P("tp", None),
        P("tp", None),
        P(SP_TP, None),
        P(),
        P(),
        P(SP, "tp"),
        P(SP, "tp"),
        P("tp", SP),
        P(),
    )
    return jax.shard_map(
        layer, mesh=split, in_specs=placed, out_specs=P(SP_TP, None), check_vma=False
    )
```

```python
import functools
import math

import jax
import jax.numpy as jnp
from jax import lax
from jax.experimental import pallas as pl
from jax.experimental.pallas import tpu as pltpu
from jax.sharding import Mesh
from jax.sharding import PartitionSpec as P


BLOCK = 512
SP = ("sp_0", "sp_1", "sp_2")
SP_TP = ("sp_0", "sp_1", "sp_2", "tp")
RING = 4
LIMIT = 16 * 1024 * 1024
EPSILON = 1e-06


def along(step):
    return [(i, (i + step) % RING) for i in range(RING)]


def role_shift(first, step):
    pairs = []
    for z in range(RING):
        for y in range(RING):
            for c in range(2):
                if (c == 0) == first:
                    to = (z, (y + step) % RING)
                else:
                    to = ((z + step) % RING, y)
                pairs.append((z * 8 + y * 2 + c, to[0] * 8 + to[1] * 2 + c))
    return pairs


def flipped(size, bit):
    return [(i, i ^ bit) for i in range(size)]


def near_shards(mine):
    near = functools.partial(role_shift, True)
    return (
        lax.ppermute(mine, SP, near(1)),
        lax.ppermute(mine, SP, near(-1)),
        lax.ppermute(mine, SP, near(2)),
    )


def far_shards(s0, s1):
    wide = functools.partial(role_shift, False)
    ra = lax.ppermute(s0, SP, wide(1))
    lb = lax.ppermute(s1, SP, wide(-1))
    fa = lax.ppermute(ra, SP, wide(1))
    fb = lax.ppermute(lb, SP, wide(-1))
    rb = lax.ppermute(s1, SP, wide(1))
    la = lax.ppermute(s0, SP, wide(-1))
    own = [s0, s1, ra, lb, fa, fb, rb, la]
    return own + [lax.ppermute(v, "sp_2", flipped(2, 1)) for v in own]


PIECES = ((0, 0), (2, 0), (0, 3), (2, 1), (0, 2), (2, 2), (2, 3), (0, 1))


def place_body(chosen, coord, *refs):
    count = 2 * len(chosen)
    pieces = refs[:count]
    w, sem = refs[-2:]
    z, y, c = coord[0], coord[1], coord[2]
    offs = (0, RING - 1, 1, 2)

    def copies(low):
        made = []
        for side in range(2):
            core = side if low else 1 - side
            for i, index in enumerate(chosen):
                first, away = PIECES[index]
                for k in range(2):
                    near = offs[first + k]
                    dz, dy = (away, near) if core == 0 else (near, away)
                    chip = ((z + dz) % RING) * RING + (y + dy) % RING
                    src = pieces[side * len(chosen) + i].at[k]
                    made.append(
                        pltpu.make_async_copy(src, w.at[:, chip, core], sem.at[len(made)])
                    )
        return made

    for low in (True, False):

        @pl.when((c == 0) == low)
        def _():
            made = copies(low)
            for one in made:
                one.start()
            for one in made:
                one.wait()


def place(coord, weights, chosen, w=None):
    n = len(PIECES)
    pieces = [weights[side * n + i] for side in range(2) for i in chosen]
    width = weights[0].shape[-1]
    hb = pl.BlockSpec(memory_space=pltpu.HBM)
    vm = pl.BlockSpec(memory_space=pltpu.VMEM)
    more = [] if w is None else [w]
    return pl.pallas_call(
        functools.partial(place_body, chosen),
        out_shape=jax.ShapeDtypeStruct((3, 16, 2, 64, width), jnp.bfloat16),
        in_specs=[pl.BlockSpec(memory_space=pltpu.SMEM)] + [hb] * len(pieces) + [vm] * len(more),
        out_specs=vm,
        scratch_shapes=[pltpu.SemaphoreType.DMA((2 * len(pieces),))],
        input_output_aliases={} if w is None else {1 + len(pieces): 0},
        compiler_params=pltpu.CompilerParams(vmem_limit_bytes=LIMIT),
    )(coord, *pieces, *more)


def ffn_body(n_in, n_out, *refs):
    xs = refs[:n_in]
    w = refs[n_in]
    outs = refs[n_in + 1 : n_in + 1 + n_out]
    x, both, hid = refs[n_in + 1 + n_out :]
    rows, model = x.shape
    width = both.shape[2]
    per = rows // n_in
    for i in range(n_in):
        x[i * per : (i + 1) * per, :] = xs[i][...]

    def enter(i, carry):
        both[i] = jnp.dot(x[...], w[i].reshape(model, width), preferred_element_type=jnp.float32)
        return carry

    lax.fori_loop(0, 2, enter, 0)
    g = both[0]
    hid[...] = (g * (1.0 / (1.0 + jnp.exp(-g))) * both[1]).astype(jnp.bfloat16)
    per_out = rows // n_out
    step = 256
    turns = 2

    def leave(turn, carry):
        for j in range(model // step // turns):
            k = turn * (model // step // turns) + j
            part = lax.dot_general(
                hid[...],
                w[2, pl.ds(2 * k, 2)].reshape(step, width),
                (((1,), (1,)), ((), ())),
                preferred_element_type=jnp.float32,
            ).astype(jnp.bfloat16)
            for i in range(n_out):
                outs[i][:, pl.ds(pl.multiple_of(k * step, step), step)] = part[
                    i * per_out : (i + 1) * per_out
                ]
        return carry

    lax.fori_loop(0, turns, leave, 0)


def ffn(w, xs, n_out):
    rows = sum(v.shape[0] for v in xs)
    model = xs[0].shape[1]
    width = w.shape[-1]
    vm = pl.BlockSpec(memory_space=pltpu.VMEM)
    return pl.pallas_call(
        functools.partial(ffn_body, len(xs), n_out),
        out_shape=[jax.ShapeDtypeStruct((rows // n_out, model), jnp.bfloat16)] * n_out,
        in_specs=[vm] * (len(xs) + 1),
        out_specs=[vm] * n_out,
        scratch_shapes=[
            pltpu.VMEM((rows, model), jnp.bfloat16),
            pltpu.VMEM((2, rows, width), jnp.float32),
            pltpu.VMEM((rows, width), jnp.bfloat16),
        ],
        compiler_params=pltpu.CompilerParams(vmem_limit_bytes=LIMIT),
        name="ffn_rows",
    )(*xs, w)


def summed_decay(ld, scratch, span):
    scratch[...] = jnp.zeros_like(scratch)
    scratch[0:2, :] = ld[...]
    v = scratch[0:8, :]
    lane = lax.broadcasted_iota(jnp.int32, v.shape, 1) % span
    step = 1
    while step < span:
        v = v + jnp.where(lane >= step, pltpu.roll(v, step, 1), 0.0)
        step *= 2
    scratch[0:8, :] = v
    return v, scratch[...].T


def times_wide(q, state):
    high = state.astype(jnp.bfloat16)
    low = (state - high.astype(jnp.float32)).astype(jnp.bfloat16)
    return jnp.dot(q, high, preferred_element_type=jnp.float32) + jnp.dot(
        q, low, preferred_element_type=jnp.float32
    )


def block_state(row, col, k, v, h, b, depth):
    lanes = slice(h * depth, (h + 1) * depth)
    here = slice(b * BLOCK, (b + 1) * BLOCK)
    last = row[h : h + 1, (b + 1) * BLOCK - 1 : (b + 1) * BLOCK]
    to_end = jnp.exp(last - col[here, h : h + 1]) * depth ** (-0.5)
    scaled = (k[here, lanes].astype(jnp.float32) * to_end).astype(jnp.bfloat16)
    added = lax.dot_general(
        scaled, v[here, lanes], (((0,), (0,)), ((), ())), preferred_element_type=jnp.float32
    )
    return added, last


def state_body(ld, k, v, message, scratch):
    rows, heads, depth = k.shape[0], ld.shape[0], message.shape[2]
    row, col = summed_decay(ld, scratch, BLOCK)
    for h in range(heads):
        state, total = block_state(row, col, k, v, h, 0, depth)
        for b in range(1, rows // BLOCK):
            added, last = block_state(row, col, k, v, h, b, depth)
            state = jnp.exp(last) * state + added
            total = total + last
        write_state(message, h, jnp.broadcast_to(jnp.exp(total), (1, depth)), state)


def joining(one, other, out, sem):
    made = [pltpu.make_async_copy(r, out.at[i], sem.at[i]) for i, r in enumerate((one, other))]
    for copy in made:
        copy.start()
    return made


def within_body(ld, q, k, v, near, far, out, both, scratch, sem):
    rows, heads = q.shape[0], ld.shape[0]
    depth = q.shape[1] // heads
    copies = joining(near, far, both, sem)
    row, col = summed_decay(ld, scratch, BLOCK)
    scale = depth ** (-0.5)
    tile = BLOCK // 2
    causal = lax.broadcasted_iota(jnp.int32, (tile, tile), 0) >= lax.broadcasted_iota(
        jnp.int32, (tile, tile), 1
    )
    for h in range(heads):
        lanes = slice(h * depth, (h + 1) * depth)
        state = None
        for b in range(rows // BLOCK):
            for i in range(2):
                t0 = b * BLOCK + i * tile
                seen = slice(b * BLOCK, t0 + tile)
                here = slice(t0, t0 + tile)
                span = (i + 1) * tile
                products = lax.dot_general(
                    q[here, lanes],
                    k[seen, lanes],
                    (((1,), (1,)), ((), ())),
                    preferred_element_type=jnp.float32,
                )
                gap = (col[here, h : h + 1] + math.log(scale)) - row[h : h + 1, seen]
                edge = jnp.where(causal, gap[:, span - tile :], -jnp.inf)
                gap = edge if i == 0 else jnp.concatenate([gap[:, : span - tile], edge], axis=1)
                scores = (products * jnp.exp(gap)).astype(jnp.bfloat16)
                result = jnp.dot(scores, v[seen, lanes], preferred_element_type=jnp.float32)
                if b > 0:
                    result = result + times_wide(q[here, lanes], state) * jnp.exp(
                        col[here, h : h + 1]
                    )
                out[here, lanes] = result
            if b + 1 < rows // BLOCK:
                added, last = block_state(row, col, k, v, h, b, depth)
                state = added if b == 0 else jnp.exp(last) * state + added
    for copy in copies:
        copy.wait()


def finish_body(coord, ld, q, within, gates, before, far3, far2, far1, gain, w_near, w_far, o0, o1, o2, o3, both, scratch, sums, sem):
    rows, heads, depth = q.shape[0], ld.shape[0], before.shape[2]
    copies = joining(w_near, w_far, both, sem)
    _, sums[...] = summed_decay(ld, scratch, rows)
    states = []
    for h in range(heads):
        state = read_state(far3, h)[1]
        for ref in (far2, far1):
            decay, more = read_state(ref, h)
            state = decay * state + more
        states.append(before[h, depth : depth + 1, :] * state + before[h, 0:depth, :])
    quarter = rows // RING
    for k, out in enumerate((o0, o1, o2, o3)):
        here = pl.ds(pl.multiple_of(((coord[3] + k) % RING) * quarter, quarter), quarter)
        for h in range(heads):
            lanes = slice(h * depth, (h + 1) * depth)
            retention = within[here, lanes] + times_wide(q[here, lanes], states[h]) * jnp.exp(
                sums[here, h : h + 1]
            )
            centered = retention - jnp.mean(retention, axis=-1, keepdims=True)
            variance = jnp.mean(centered * centered, axis=-1, keepdims=True)
            normed = centered * lax.rsqrt(variance + EPSILON) * gain[h : h + 1, :]
            g = gates[here, lanes].astype(jnp.float32)
            out[:, lanes] = (g * (1.0 / (1.0 + jnp.exp(-g))) * normed).astype(jnp.bfloat16)
    for copy in copies:
        copy.wait()


def vmem_call(body, out_shape, *args, scratch=(), smem=0, hbm=(), hbm_out=()):
    vm = pl.BlockSpec(memory_space=pltpu.VMEM)
    hb = pl.BlockSpec(memory_space=pltpu.HBM)
    sm = pl.BlockSpec(memory_space=pltpu.SMEM)
    specs = [sm if i < smem else hb if i in hbm else vm for i in range(len(args))]
    if isinstance(out_shape, tuple):
        out_specs = tuple(hb if i in hbm_out else vm for i in range(len(out_shape)))
    else:
        out_specs = vm
    return pl.pallas_call(
        body,
        out_shape=out_shape,
        in_specs=specs,
        out_specs=out_specs,
        scratch_shapes=list(scratch),
        compiler_params=pltpu.CompilerParams(vmem_limit_bytes=LIMIT),
    )(*args)


def mix_body(coord, r0, r1, r2, r3, own, near, near2, far, far2, resid, gain1, gain2, middle, out_a, out_b):
    half = own.shape[0] // 2
    low = coord[2] == 0

    def chosen(one, other):
        return jnp.where(low, one.astype(jnp.float32), other.astype(jnp.float32)).astype(jnp.bfloat16)

    left, right = r1[...], r3[...]
    far_a, far_b = r2[:, 0:half], r2[:, half:]
    columns = [
        r0[...],
        chosen(left, right),
        chosen(right, left),
        chosen(far_a, far_b),
        chosen(far_b, far_a),
    ]
    rows = [v[...] for v in (own, near, near2, far, far2)]
    mixed = jnp.dot(
        jnp.concatenate(columns, axis=1),
        jnp.concatenate(rows, axis=0),
        preferred_element_type=jnp.float32,
    )
    mixed = mixed.astype(jnp.bfloat16).astype(jnp.float32)
    mean = jnp.mean(mixed * mixed, axis=-1, keepdims=True)
    mid = resid[...].astype(jnp.float32) + mixed * lax.rsqrt(mean + EPSILON) * gain1[...]
    mid = mid.astype(jnp.bfloat16)
    middle[...] = mid
    mid = mid.astype(jnp.float32)
    mean = jnp.mean(mid * mid, axis=-1, keepdims=True)
    h = (mid * lax.rsqrt(mean + EPSILON) * gain2[...]).astype(jnp.bfloat16)
    out_a[...] = h[: h.shape[0] // 2]
    out_b[...] = h[h.shape[0] // 2 :]


def final_body(own_a, own_b, sum_a, sum_b, near_a, near_b, middle, gain, out, rows, sem):
    half = own_a.shape[0]
    step = half // 2
    copies = []
    for i, refs in enumerate(((own_a, sum_a, near_a), (own_b, sum_b, near_b))):
        for j in range(2):
            part = slice(j * step, (j + 1) * step)
            here = slice(i * half + j * step, i * half + (j + 1) * step)
            total = sum(r[part, :].astype(jnp.float32) for r in refs)
            total = total.astype(jnp.bfloat16).astype(jnp.float32)
            mean = jnp.mean(total * total, axis=-1, keepdims=True)
            mid = middle[here, :].astype(jnp.float32)
            done = mid + total * lax.rsqrt(mean + EPSILON) * gain[...]
            rows[here, :] = done.astype(jnp.bfloat16)
            copy = pltpu.make_async_copy(rows.at[here], out.at[here], sem.at[2 * i + j])
            copy.start()
            copies.append(copy)
    for copy in copies:
        copy.wait()


def read_state(ref, h):
    depth = ref.shape[2]
    state = ref[h, 0:depth, :].astype(jnp.float32)
    if ref.dtype == jnp.float32:
        return ref[h, depth : depth + 1, :], state
    tail = ref[h, depth : depth + 16, :].astype(jnp.float32)
    return tail[0:1] + tail[1:2], state


def write_state(ref, h, decay, state):
    depth = ref.shape[2]
    if ref.dtype == jnp.float32:
        ref[h, 0:depth, :] = state
        ref[h, depth : depth + 8, :] = jnp.broadcast_to(decay, (8, depth))
        return
    wide = jnp.broadcast_to(decay, (16, depth))
    high = wide.astype(jnp.bfloat16)
    low = (wide - high.astype(jnp.float32)).astype(jnp.bfloat16)
    at = lax.broadcasted_iota(jnp.int32, (16, depth), 0)
    ref[h, 0:depth, :] = state.astype(jnp.bfloat16)
    ref[h, depth : depth + 16, :] = jnp.where(at == 0, high, low)


def joined(earlier, later):
    return (earlier[0] * later[0], later[0] * earlier[1] + later[1])


def either(flag, one, other):
    return tuple(jnp.where(flag, a, b) for a, b in zip(one, other))


def pair_body(coord, own, got, before, message):
    upper = coord[2] == 1
    for h in range(own.shape[0]):
        mine, other = read_state(own, h), read_state(got, h)
        nothing = (jnp.ones_like(mine[0]), jnp.zeros_like(mine[1]))
        both = either(upper, joined(other, mine), joined(mine, other))
        write_state(message, h, *both)
        write_state(before, h, *either(upper, other, nothing))


def plane_body(coord, own, inner, b1, b2, b3, before, message):
    y = coord[1]
    for h in range(own.shape[0]):
        mine = read_state(own, h)
        nothing = (jnp.ones_like(mine[0]), jnp.zeros_like(mine[1]))
        back = [read_state(r, h) for r in (b1, b2, b3)]
        past = nothing
        for k in (3, 2, 1):
            past = joined(past, either(y >= k, back[k - 1], nothing))
        whole = joined(past, mine)
        for k in (3, 2, 1):
            whole = joined(whole, either(y < k, back[k - 1], nothing))
        write_state(message, h, *whole)
        write_state(before, h, *joined(past, read_state(inner, h)))


def kernel(body, out_shape, *args, **more):
    return vmem_call(body, out_shape, *args, **more)


def shaped(dtype, *dims):
    return jax.ShapeDtypeStruct(dims, dtype)


def layer(
    queries,
    keys,
    values,
    gates,
    log_decay,
    norm_gain,
    out_weight,
    resid,
    post_mix_gain,
    pre_ffn_gain,
    w_gate,
    w_up,
    w_down,
    post_ffn_gain,
):
    f32, bf16 = jnp.float32, jnp.bfloat16
    z, y, c = (lax.axis_index(a) for a in SP)
    x = lax.axis_index("tp")
    coord = jnp.stack([z, y, c, x]).astype(jnp.int32)
    up1, down1 = along(1), along(-1)
    o_half = out_weight.shape[0] // 2
    turn = [(i, (i + 1) % RING) for i in range(RING)]
    turn += [(RING + i, RING + (i - 1) % RING) for i in range(RING)]
    o_near = lax.ppermute(out_weight, ("sp_2", "tp"), turn)
    o_fore = lax.dynamic_slice_in_dim(o_near, c * o_half, o_half, 0)
    o_far = lax.ppermute(o_fore, ("sp_2", "tp"), turn)
    o_near2 = lax.ppermute(o_near, "sp_2", flipped(2, 1))
    o_far2 = lax.ppermute(o_far, "sp_2", flipped(2, 1))

    rows, width = queries.shape
    heads = log_decay.shape[1]
    depth = width // heads
    ld = log_decay.T
    sums = pltpu.VMEM((128, rows), f32)
    total_shape = shaped(f32, heads, depth + 8, depth)
    message_shape = shaped(bf16, heads, depth + 16, depth)
    block = w_gate.shape
    mine = jnp.stack([w_gate, w_up, w_down.T])
    message = kernel(state_body, message_shape, ld, keys, values, scratch=(sums,))
    w_right, w_left, w_far = near_shards(mine)
    pair = pltpu.SemaphoreType.DMA((2,))
    within, s0 = kernel(
        within_body,
        (shaped(f32, rows, width), shaped(bf16, 2, 3, *block)),
        ld, queries, keys, values, mine, w_right,
        scratch=(sums, pair),
        hbm=(4, 5),
        hbm_out=(1,),
    )
    got = lax.ppermute(message, "sp_2", flipped(2, 1))
    inner, message = kernel(pair_body, (total_shape, message_shape), coord, message, got, smem=1)
    back = [lax.ppermute(message, "sp_1", along(k)) for k in (1, 2, 3)]
    before, message = kernel(
        plane_body, (total_shape, message_shape), coord, message, inner, *back, smem=1
    )
    back = [lax.ppermute(message, "sp_0", [(i, i + k) for i in range(RING - k)]) for k in (3, 2, 1)]
    quarter, model = resid.shape
    piece = shaped(bf16, quarter, width)
    *turned, s1 = kernel(
        finish_body,
        (piece,) * RING + (shaped(bf16, 2, 3, *block),),
        coord, ld, queries, within, gates, before, *back, norm_gain, w_left, w_far,
        scratch=(sums, pltpu.VMEM((rows, 128), f32), pair),
        smem=1,
        hbm=(10, 11),
        hbm_out=(4,),
    )
    weights = far_shards(s0, s1)
    turned = (turned[0], *(lax.ppermute(turned[k], "tp", along(k)) for k in (1, 2, 3)))
    half = quarter // 2
    middle, h_a, h_b = kernel(
        mix_body,
        (shaped(bf16, quarter, model), shaped(bf16, half, model), shaped(bf16, half, model)),
        coord, *turned, out_weight, o_near, o_near2, o_far, o_far2, resid,
        post_mix_gain.reshape(1, -1), pre_ffn_gain.reshape(1, -1),
        smem=1,
    )

    r_a = lax.ppermute(h_a, "tp", up1)
    l_b = lax.ppermute(h_b, "tp", down1)
    far_a = lax.ppermute(r_a, "tp", up1)
    far_b = lax.ppermute(l_b, "tp", down1)
    r_b = lax.ppermute(h_b, "tp", up1)
    l_a = lax.ppermute(h_a, "tp", down1)

    w = place(coord, weights, (0, 1, 2, 3, 6, 7))
    w = place(coord, weights, (4, 5), w)

    def feed(*xs):
        return ffn(w, xs, 2)

    right_a, left_b = feed(r_a, l_b)
    opp_a, opp_b = feed(far_a, far_b)
    right_b, left_a = feed(r_b, l_a)
    own_a, own_b = feed(h_a, h_b)
    near_b = lax.ppermute(left_b, "tp", up1)
    near_a = lax.ppermute(right_a, "tp", down1)
    far_in_a = lax.ppermute(opp_a, "tp", up1)
    far_in_b = lax.ppermute(opp_b, "tp", down1)
    wide = lambda v: v.astype(f32)
    sum_a = lax.ppermute((wide(left_a) + wide(far_in_a)).astype(bf16), "tp", up1)
    sum_b = lax.ppermute((wide(right_b) + wide(far_in_b)).astype(bf16), "tp", down1)
    (updated,) = kernel(
        final_body,
        (shaped(bf16, quarter, model),),
        own_a, own_b, sum_a, sum_b, near_a, near_b, middle, post_ffn_gain.reshape(1, -1),
        scratch=(pltpu.VMEM((quarter, model), bf16), pltpu.SemaphoreType.DMA((4,))),
        hbm_out=(0,),
    )
    return updated


def solution(mesh):
    split = Mesh(mesh.devices.reshape(4, 4, 2, mesh.shape["tp"]), ("sp_0", "sp_1", "sp_2", "tp"))
    placed = (
        P(SP, "tp"),
        P(SP, "tp"),
        P(SP, "tp"),
        P(SP, "tp"),
        P(SP, "tp"),
        P("tp", None),
        P("tp", None),
        P(SP_TP, None),
        P(),
        P(),
        P(SP, "tp"),
        P(SP, "tp"),
        P("tp", SP),
        P(),
    )
    return jax.shard_map(
        layer, mesh=split, in_specs=placed, out_specs=P(SP_TP, None), check_vma=False
    )
```
